32 devices in a mesh: ep: 4 (over y, x), tp: 8 (over z, core).
Axes of the slice: x: 2, y: 2, z: 4, core: 2. Of those that a mesh axis runs over, the one named last changes fastest.
Arguments:
- q_latent: bfloat16 [4096, 512], P('ep'), may hold values from -6 to 6
- kv_latent: bfloat16 [4096, 256], P('ep'), may hold values from -6 to 6
- rope_key: bfloat16 [4096, 32], P('ep'), may hold values from -1200 to 1200
- q_gain: float32 [512], replicated, may hold values from 0.1 to 1.9
- kv_gain: float32 [256], replicated, may hold values from 0.1 to 1.9
- w_query: bfloat16 [512, 1536], P(None, 'tp'), may hold values from -0.25 to 0.25
- w_keyval: bfloat16 [256, 2048], P(None, 'tp'), may hold values from -0.375 to 0.375
- w_output: bfloat16 [1024, 2048], P(None, 'tp'), may hold values from -0.1875 to 0.1875
- moe_input: bfloat16 [1024, 2048], P('ep'), may hold values from -6 to 6
- moe_gain: float32 [2048], replicated, may hold values from 0.1 to 1.9
- routes: int32 [1024, 2], P('ep'), may hold values from 0 to 3, all different within a row; in each aligned block of 32 rows (0 to 31, 32 to 63, ...) at most 24 rows name the same one
- route_weight: float32 [1024, 2], P('ep'), may hold values from 0.25 to 2
- expert_gate: bfloat16 [4, 2048, 4096], P('ep', None, 'tp'), may hold values from -0.125 to 0.125
- expert_up: bfloat16 [4, 2048, 4096], P('ep', None, 'tp'), may hold values from -0.125 to 0.125
- expert_down: bfloat16 [4, 4096, 2048], P('ep', 'tp'), may hold values from -0.09375 to 0.09375
- shared_gate: bfloat16 [2048, 2048], P(None, 'tp'), may hold values from -0.125 to 0.125
- shared_up: bfloat16 [2048, 2048], P(None, 'tp'), may hold values from -0.125 to 0.125
- shared_down: bfloat16 [2048, 2048], P('tp'), may hold values from -0.125 to 0.125
Outputs:
- mixed: bfloat16 [4096, 2048], P('ep', 'tp')
- moe_out: bfloat16 [1024, 2048], P(('ep', 'tp'))
The draws below stay inside these ranges and needn't reach their ends.
Inputs may be any that keep to these rules, and one draw needn't show every extreme that they name: `routes`: in each aligned block of 32 rows (the rows of one device's output) no expert is named by more than 24 rows, a bound that some block reaches. Each row names 2 different experts.
All inputs are finite; a program needn't handle non-finite values.
Results may differ from the reference program's by a relative error of at most 0.023.
Values may be sent and summed in bfloat16 or wider, within the bound.
A program may use at most 128 MiB of HBM per device.

```python
import math
import jax
import jax.numpy as jnp
import numpy as np
from jax import lax

D = 2048
HEADS = 16
NOPE = 64
ROPE_DIM = 32
VDIM = 64
QLAT = 512
KVLAT = 256
TOKA_EP = 1024
TOK_A = 4096
MOE_DEV = 32
TOK_B = 1024
EXPERTS = 4
FE = 4096
FS = 2048
FE_PART = 512
FS_PART = 256
TOP = 2
CAP = 24
N_EP = 4
N_TP = 8


def draw_rope_key(key, part):
    drawn = jax.random.normal(jax.random.fold_in(key, 11), (TOK_A, ROPE_DIM), jnp.float32)
    drawn = jnp.clip(drawn, -6.0, 6.0)
    return drawn.astype(jnp.bfloat16)


def block_scale(own_key, extent, split, smallest, top_value):
    level = 1.0
    for axis_at, parts in split:
        heights = jax.random.uniform(jax.random.fold_in(jax.random.fold_in(own_key, 6), axis_at), (parts,), jnp.float32, smallest / len(split), top_value / len(split))
        level = level * jnp.repeat(jnp.exp(heights), extent[axis_at] // parts).reshape((-1,) + (1,) * (len(extent) - 1 - axis_at))
    return level


def routed_block(own_key, own, number, rows, amount, top, bound, skew):
    order = jax.random.permutation(own_key, amount)
    packed, ordinary = shares(amount, rows * top, bound, skew, True), shares(amount, rows * top, bound, skew, False)
    places = jnp.arange(amount)

    def named(lengths, offset_by):
        used = int((lengths > 0).sum())
        fixed = max(1, used // 4)
        passed = fixed + (places - fixed + offset_by * (used - fixed)) % max(1, amount - fixed)
        return jnp.zeros((amount,), jnp.int32).at[order[jnp.where(places < fixed, places, passed)]].set(jnp.asarray(lengths, jnp.int32))

    lengths = jnp.where(number % 4 == 0, named(packed, number // 4), named(ordinary, number - number // 4 - 1))
    mixed = jax.random.permutation(jax.random.fold_in(own, 3), amount)
    source_of, taker = mixed[0:amount // 2 * 2:2], mixed[1:amount // 2 * 2:2]
    room = jnp.minimum(lengths[source_of] - 1, bound - lengths[taker]) // 2
    room = jnp.where((source_of == order[0]) | (taker == order[0]) | (lengths[taker] == 0), 0, jnp.maximum(room, 0))
    passed = jax.random.randint(jax.random.fold_in(own, 4), (amount // 2,), 0, 1 << 20) % (room + 1)
    lengths = lengths.at[source_of].add(-passed).at[taker].add(passed)
    members = jnp.searchsorted(jnp.cumsum(lengths), jnp.arange(rows * top), side="right").astype(jnp.int32)
    grid = members.reshape(top, rows).T
    grid = grid[jax.random.permutation(jax.random.fold_in(own, 1), rows)]
    offset_by = jax.random.randint(jax.random.fold_in(own, 2), (rows, 1), 0, top)
    return jnp.take_along_axis(grid, (jnp.arange(top)[None, :] + offset_by) % top, axis=1)


def shares(amount, total, bound, slope, full):
    portions = [(1 << 20) // math.isqrt(rank ** slope) + 1 for rank in range(1, amount + 1)]
    largest = bound if full else min(bound, max(-(-total // amount), total * portions[0] // sum(portions)))
    least = 1 if total - largest >= amount - 1 else 0
    holding, rest = [largest] + [least] * (amount - 1), total - largest - least * (amount - 1)
    while rest > 0:
        free = [i for i in range(1, amount) if holding[i] < largest] or [i for i in range(1, amount) if holding[i] < bound]
        whole, left = sum([portions[i] for i in free]), rest
        for i in free:
            extra = min(bound - holding[i], max(1, left * portions[i] // whole), rest)
            holding[i] = holding[i] + extra
            rest = rest - extra
    return np.array(holding)


def bell_draw(key, shape, deviation, bound, pieces=(), held_as=jnp.bfloat16):
    values = jax.random.normal(key, shape, jnp.float32) * deviation
    if len(pieces) > 0:
        values = block_scale(key, shape, pieces, -0.22, 0.18) * values
    return jnp.clip(values, min=-bound, max=bound).astype(held_as)


def setup_inputs(seed: int = 0) -> dict:
    streams_of = jax.random.split(jax.random.key(seed), 19)
    q_latent = bell_draw(streams_of[0], (TOK_A, QLAT), 1.0, 6.0, ((0, 4),))
    kv_latent = bell_draw(streams_of[1], (TOK_A, KVLAT), 1.0, 6.0, ((0, 4),))
    rope_key = draw_rope_key(jax.random.fold_in(streams_of[18], 71), 0)
    q_gain = jnp.clip(1.0 + 0.18 * jax.random.normal(streams_of[3], (QLAT,), jnp.float32), 0.1, 1.9)
    kv_gain = jnp.clip(1.0 + 0.18 * jax.random.normal(streams_of[4], (KVLAT,), jnp.float32), 0.1, 1.9)
    w_query = bell_draw(streams_of[5], (QLAT, HEADS * (NOPE + ROPE_DIM)), QLAT ** -0.5, 0.25, ((1, 8),))
    w_keyval = bell_draw(streams_of[6], (KVLAT, HEADS * (NOPE + VDIM)), KVLAT ** -0.5, 0.375, ((1, 8),))
    w_output = bell_draw(streams_of[7], (HEADS * VDIM, D), (HEADS * VDIM) ** -0.5, 0.1875, ((1, 8),))
    moe_input = bell_draw(streams_of[8], (TOK_B, D), 1.0, 6.0, ((0, 4),))
    moe_gain = jnp.clip(1.0 + 0.18 * jax.random.normal(streams_of[9], (D,), jnp.float32), 0.1, 1.9)
    routes_keys = jax.random.split(jax.random.fold_in(streams_of[10], 1), TOK_B // MOE_DEV)
    routes_turns = jax.random.permutation(jax.random.fold_in(streams_of[10], 3), TOK_B // MOE_DEV)
    routes = jax.vmap(lambda own, number: routed_block(jax.random.fold_in(streams_of[10], 2), own, number, MOE_DEV, EXPERTS, TOP, CAP, 1))(routes_keys, routes_turns).reshape((TOK_B, TOP))
    route_weight = jnp.clip(0.25 + 1.75 * jax.random.uniform(streams_of[11], (TOK_B, TOP), jnp.float32) ** block_scale(streams_of[11], (TOK_B, TOP), ((0, 4),), -0.2, 0.2), 0.25, 2.0)
    expert_gate = bell_draw(streams_of[12], (EXPERTS, D, FE), D ** -0.5, 0.125, ((0, 4), (2, 8)))
    expert_up = bell_draw(streams_of[13], (EXPERTS, D, FE), D ** -0.5, 0.125, ((0, 4), (2, 8)))
    expert_down = bell_draw(streams_of[14], (EXPERTS, FE, D), FE ** -0.5, 0.09375, ((0, 4), (1, 8)))
    shared_gate = bell_draw(streams_of[15], (D, FS), D ** -0.5, 0.125, ((1, 8),))
    shared_up = bell_draw(streams_of[16], (D, FS), D ** -0.5, 0.125, ((1, 8),))
    shared_down = bell_draw(streams_of[17], (FS, D), FS ** -0.5, 0.125, ((0, 8),))
    return dict(q_latent=q_latent, kv_latent=kv_latent, rope_key=rope_key, q_gain=q_gain, kv_gain=kv_gain, w_query=w_query, w_keyval=w_keyval, w_output=w_output, moe_input=moe_input, moe_gain=moe_gain, routes=routes, route_weight=route_weight, expert_gate=expert_gate, expert_up=expert_up, expert_down=expert_down, shared_gate=shared_gate, shared_up=shared_up, shared_down=shared_down)


norm_eps = 1e-06
layer_eps = 1e-05
rotary_base = 10000.0
floor_value = -1e+30

def rms_scale(values, gain):
    widened = values.astype(jnp.float32)
    return (widened * lax.rsqrt(lax.optimization_barrier(jnp.mean(widened * widened, -1, keepdims=True)) + norm_eps) * gain).astype(jnp.bfloat16)

def layer_scale(values, gain):
    widened = values.astype(jnp.float32)
    centred = widened - lax.optimization_barrier(jnp.mean(widened, -1, keepdims=True))
    return (centred * lax.rsqrt(lax.optimization_barrier(jnp.mean(centred * centred, -1, keepdims=True)) + layer_eps) * gain).astype(jnp.bfloat16)

def rotary_tables(positions):
    halfway = ROPE_DIM // 2
    inverse = rotary_base ** (-(jnp.arange(halfway, dtype=jnp.float32) * 2.0 / ROPE_DIM))
    angles = positions.astype(jnp.float32)[:, None] * inverse[None, :]
    return (jnp.cos(angles), jnp.sin(angles))

def rotate(values, cosine_table, sine_table):
    halfway = values.shape[-1] // 2
    first_half = values[..., :halfway]
    second_half = values[..., halfway:]
    return jnp.concatenate([first_half * cosine_table - second_half * sine_table, second_half * cosine_table + first_half * sine_table], -1)

def merge_block(carried, stats):
    running_max, running_sum, running_acc = carried
    block_max, block_sum, attended = stats
    new_max = jnp.maximum(running_max, block_max)
    old_weight = jnp.exp(running_max - new_max)
    new_weight = jnp.exp(block_max - new_max)
    return (new_max, running_sum * old_weight + block_sum * new_weight, running_acc * old_weight[..., None] + attended.astype(jnp.float32) * new_weight[..., None])

def group_sum(hidden, down_weight, group_width):

    def add_group(group_index, total):
        hidden_cols = lax.dynamic_slice_in_dim(hidden, group_index * group_width, group_width, 1)
        weight_rows = lax.dynamic_slice_in_dim(down_weight, group_index * group_width, group_width, 0)
        product = jnp.dot(hidden_cols, weight_rows, preferred_element_type=jnp.float32)
        return total + lax.optimization_barrier(product.astype(jnp.bfloat16)).astype(jnp.float32)
    return lax.fori_loop(0, N_TP, add_group, jnp.zeros((hidden.shape[0], down_weight.shape[1]), jnp.float32))

def reference(q_latent, kv_latent, rope_key, q_gain, kv_gain, w_query, w_keyval, w_output, moe_input, moe_gain, routes, route_weight, expert_gate, expert_up, expert_down, shared_gate, shared_up, shared_down):
    positions = jnp.arange(TOK_A, dtype=jnp.int32)
    cosine_table, sine_table = rotary_tables(positions)
    q_normed = rms_scale(q_latent, q_gain)
    kv_normed = rms_scale(kv_latent, kv_gain)
    key_rot = rotate(rope_key.astype(jnp.float32), cosine_table, sine_table).astype(jnp.bfloat16)
    projected = jnp.dot(q_normed, w_query, preferred_element_type=jnp.float32).reshape(TOK_A, HEADS, NOPE + ROPE_DIM)
    queries = jnp.concatenate([projected[..., :NOPE], rotate(projected[..., NOPE:], cosine_table[:, None, :], sine_table[:, None, :])], -1).astype(jnp.bfloat16)
    keyvals = jnp.dot(kv_normed, w_keyval, preferred_element_type=jnp.float32).astype(jnp.bfloat16)
    keyvals = keyvals.reshape(TOK_A, HEADS, NOPE + VDIM)
    scale = float(NOPE + ROPE_DIM) ** (-0.5)

    def visit_group(group_index):
        first_row = group_index * TOKA_EP
        query_block = lax.dynamic_slice_in_dim(queries, first_row, TOKA_EP, 0).astype(jnp.float32)
        query_pos = first_row + jnp.arange(TOKA_EP, dtype=jnp.int32)

        def visit_block(block_index, carried):
            key_first = block_index * TOKA_EP
            keyval_block = lax.dynamic_slice_in_dim(keyvals, key_first, TOKA_EP, 0).astype(jnp.float32)
            rotated_block = lax.dynamic_slice_in_dim(key_rot, key_first, TOKA_EP, 0).astype(jnp.float32)
            key_pos = key_first + jnp.arange(TOKA_EP, dtype=jnp.int32)
            scores = jnp.einsum('qhd,khd->hqk', query_block[..., :NOPE], keyval_block[..., :NOPE])
            scores = (scores + jnp.einsum('qhd,kd->hqk', query_block[..., NOPE:], rotated_block)) * scale
            allowed = key_pos[None, :] <= query_pos[:, None]
            scores = jnp.where(allowed[None], scores, -jnp.inf)
            block_max = lax.optimization_barrier(jnp.max(scores, -1))
            weights = jnp.exp(scores - block_max[..., None])
            block_sum = lax.optimization_barrier(jnp.sum(weights, -1))
            rounded = lax.optimization_barrier(weights.astype(jnp.bfloat16)).astype(jnp.float32)
            attended = jnp.einsum('hqk,khd->qhd', rounded, keyval_block[..., NOPE:])
            attended = lax.optimization_barrier(attended.astype(jnp.bfloat16)).astype(jnp.float32)
            return merge_block(carried, (block_max.T, block_sum.T, attended))
        initial = (jnp.full((TOKA_EP, HEADS), floor_value, jnp.float32), jnp.zeros((TOKA_EP, HEADS), jnp.float32), jnp.zeros((TOKA_EP, HEADS, VDIM), jnp.float32))
        running_max, running_sum, running_acc = lax.fori_loop(0, group_index + 1, visit_block, initial)
        return (running_acc / running_sum[..., None]).astype(jnp.bfloat16).reshape(TOKA_EP, HEADS * VDIM)
    heads_out = lax.map(visit_group, jnp.arange(N_EP, dtype=jnp.int32)).reshape(TOK_A, HEADS * VDIM)
    mixed = jnp.dot(heads_out, w_output, preferred_element_type=jnp.float32).astype(jnp.bfloat16)
    block_total = TOK_B // MOE_DEV
    normed = layer_scale(moe_input, moe_gain)
    entries = routes.reshape(block_total, MOE_DEV * TOP)
    onehot = (entries[..., None] == jnp.arange(EXPERTS, dtype=jnp.int32)).astype(jnp.int32)
    earlier = jnp.cumsum(onehot, 1) - onehot
    rank_in = lax.optimization_barrier(jnp.sum(earlier * onehot, -1))
    block_ids = jnp.broadcast_to(jnp.arange(block_total, dtype=jnp.int32)[:, None], entries.shape)
    token_ids = (jnp.arange(TOK_B * TOP, dtype=jnp.int32) // TOP).reshape(block_total, MOE_DEV * TOP)
    table = jnp.full((EXPERTS, block_total, CAP), -1, jnp.int32).at[entries, block_ids, rank_in].set(token_ids)

    def run_expert(operands):
        slot_token, gate_weight, up_weight, down_weight = operands
        inputs = jnp.where((slot_token >= 0)[:, None], normed[jnp.maximum(slot_token, 0)], jnp.zeros((), jnp.bfloat16))
        hidden = jax.nn.silu(jnp.dot(inputs, gate_weight, preferred_element_type=jnp.float32))
        hidden = (hidden * jnp.dot(inputs, up_weight, preferred_element_type=jnp.float32)).astype(jnp.bfloat16)
        return group_sum(hidden, down_weight, FE_PART)
    expert_sums = lax.map(run_expert, (table.reshape(EXPERTS, block_total * CAP), expert_gate, expert_up, expert_down))
    slot_of = ((entries * block_total + block_ids) * CAP + rank_in).reshape(TOK_B, TOP)
    picked = expert_sums.reshape(EXPERTS * block_total * CAP, D)[slot_of]
    routed = lax.optimization_barrier(jnp.sum(route_weight[..., None] * picked, 1))
    shared_hidden = jax.nn.silu(jnp.dot(normed, shared_gate, preferred_element_type=jnp.float32))
    shared_hidden = (shared_hidden * jnp.dot(normed, shared_up, preferred_element_type=jnp.float32)).astype(jnp.bfloat16)
    shared_total = group_sum(shared_hidden, shared_down, FS_PART)
    moe_out = (routed + shared_total).astype(jnp.bfloat16)
    return (mixed, moe_out)
```

```python
import jax
import jax.numpy as jnp
import numpy as np
from jax import lax
from jax.experimental import pallas as pl
from jax.experimental.pallas import tpu as pltpu
from jax.sharding import PartitionSpec as P

NOPE = 64
ROPE_DIM = 32
VDIM = 64
MOE_DEV = 32


norm_eps = 1e-06
layer_eps = 1e-05
rotary_base = 10000.0
floor_value = -1e30


def rms_scale(values, gain):
    widened = values.astype(jnp.float32)
    return (
        widened * lax.rsqrt(jnp.mean(widened * widened, -1, keepdims=True) + norm_eps) * gain
    ).astype(jnp.bfloat16)


def layer_scale(values, gain):
    widened = values.astype(jnp.float32)
    centred = widened - jnp.mean(widened, -1, keepdims=True)
    return (
        centred * lax.rsqrt(jnp.mean(centred * centred, -1, keepdims=True) + layer_eps) * gain
    ).astype(jnp.bfloat16)


def rotary_tables(positions):
    halfway = ROPE_DIM // 2
    inverse = rotary_base ** (-(jnp.arange(halfway, dtype=jnp.float32) * 2.0 / ROPE_DIM))
    angles = positions.astype(jnp.float32)[:, None] * inverse[None, :]
    return (jnp.cos(angles), jnp.sin(angles))


def rotate(values, cosine_table, sine_table):
    halfway = values.shape[-1] // 2
    first_half = values[..., :halfway]
    second_half = values[..., halfway:]
    return jnp.concatenate(
        [
            first_half * cosine_table - second_half * sine_table,
            second_half * cosine_table + first_half * sine_table,
        ],
        -1,
    )


def block_stats(query_block, query_pos, keyvals, rotated_keys, key_pos):
    scale = float(NOPE + ROPE_DIM) ** (-0.5)
    scores = jnp.einsum(
        "qhd,khd->hqk",
        query_block[..., :NOPE],
        keyvals[..., :NOPE],
        preferred_element_type=jnp.float32,
    )
    scores = (
        scores
        + jnp.einsum(
            "qhd,kd->hqk", query_block[..., NOPE:], rotated_keys, preferred_element_type=jnp.float32
        )
    ) * scale
    allowed = key_pos[None, :] <= query_pos[:, None]
    scores = jnp.where(allowed[None], scores, -jnp.inf)
    block_max = jnp.max(scores, -1)
    weights = jnp.exp(scores - block_max[..., None])
    block_sum = jnp.sum(weights, -1)
    attended = jnp.einsum(
        "hqk,khd->qhd",
        weights.astype(jnp.bfloat16),
        keyvals[..., NOPE:],
        preferred_element_type=jnp.float32,
    ).astype(jnp.bfloat16)
    return (block_max.T, block_sum.T, attended)


def merge_block(carried, stats):
    running_max, running_sum, running_acc = carried
    block_max, block_sum, attended = stats
    new_max = jnp.maximum(running_max, block_max)
    old_weight = jnp.exp(running_max - new_max)
    new_weight = jnp.exp(block_max - new_max)
    return (
        new_max,
        running_sum * old_weight + block_sum * new_weight,
        running_acc * old_weight[..., None] + attended.astype(jnp.float32) * new_weight[..., None],
    )


def body(
    q_latent,
    kv_latent,
    rope_key,
    q_gain,
    kv_gain,
    w_query,
    w_keyval,
    w_output,
    moe_input,
    moe_gain,
    routes,
    route_weight,
    expert_gate,
    expert_up,
    expert_down,
    shared_gate,
    shared_up,
    shared_down,
):
    row_count = q_latent.shape[0]
    own_index = lax.axis_index("ep")
    ep_count = lax.axis_size("ep")
    tp_count = lax.axis_size("tp")
    positions = own_index * row_count + jnp.arange(row_count, dtype=jnp.int32)
    cosine_table, sine_table = rotary_tables(positions)
    q_normed = rms_scale(q_latent, q_gain)
    kv_normed = rms_scale(kv_latent, kv_gain)
    key_rotated = rotate(rope_key.astype(jnp.float32), cosine_table, sine_table).astype(
        jnp.bfloat16
    )
    heads_local = w_query.shape[1] // (NOPE + ROPE_DIM)
    projected = jnp.dot(q_normed, w_query, preferred_element_type=jnp.float32)
    projected = projected.reshape(row_count, heads_local, NOPE + ROPE_DIM)
    queries = jnp.concatenate(
        [
            projected[..., :NOPE],
            rotate(projected[..., NOPE:], cosine_table[:, None, :], sine_table[:, None, :]),
        ],
        -1,
    ).astype(jnp.bfloat16)

    def expand_keys(latent_rows):
        expanded = jnp.dot(latent_rows, w_keyval, preferred_element_type=jnp.float32).astype(
            jnp.bfloat16
        )
        return expanded.reshape(latent_rows.shape[0], heads_local, NOPE + VDIM)

    initial = (
        jnp.full((row_count, heads_local), floor_value, jnp.float32),
        jnp.zeros((row_count, heads_local), jnp.float32),
        jnp.zeros((row_count, heads_local, VDIM), jnp.float32),
    )
    carried = initial
    latent_piece = lax.all_gather(kv_normed, "ep", axis=0, tiled=True)
    rotated_piece = lax.all_gather(key_rotated, "ep", axis=0, tiled=True)
    block_count = latent_piece.shape[0] // row_count

    def visit_block(inner, offset):

        def live(current):
            latent_rows = lax.dynamic_slice_in_dim(latent_piece, offset * row_count, row_count, 0)
            rotated_rows = lax.dynamic_slice_in_dim(rotated_piece, offset * row_count, row_count, 0)
            key_pos = offset * row_count + jnp.arange(row_count, dtype=jnp.int32)
            stats = block_stats(queries, positions, expand_keys(latent_rows), rotated_rows, key_pos)
            return merge_block(current, stats)

        def skipped(current):
            return current

        return (lax.cond(offset <= own_index, live, skipped, inner), None)

    carried, unused = lax.scan(visit_block, carried, jnp.arange(block_count, dtype=jnp.int32))
    running_max, running_sum, running_acc = carried
    heads_out = (
        (running_acc / running_sum[..., None])
        .astype(jnp.bfloat16)
        .reshape(row_count, heads_local * VDIM)
    )
    mixed = jnp.dot(
        lax.all_gather(heads_out, "tp", axis=1, tiled=True),
        w_output,
        preferred_element_type=jnp.float32,
    )
    mixed = mixed.astype(jnp.bfloat16)
    width = moe_input.shape[1]
    top_count = routes.shape[1]
    local_experts = expert_gate.shape[0]
    expert_count = local_experts * ep_count
    capacity = max(2, 3 * MOE_DEV * top_count // (2 * expert_count))
    normed = layer_scale(moe_input, moe_gain)
    entries = routes.reshape(tp_count, MOE_DEV * top_count)
    onehot = (entries[..., None] == jnp.arange(expert_count, dtype=jnp.int32)).astype(jnp.int32)
    earlier = jnp.cumsum(onehot, 1) - onehot
    rank_in = jnp.sum(earlier * onehot, -1)
    block_ids = jnp.arange(tp_count, dtype=jnp.int32)[:, None]
    slot_of = ((entries * tp_count + block_ids) * capacity + rank_in).reshape(-1, top_count)
    token_ids = jnp.arange(tp_count * MOE_DEV * top_count, dtype=jnp.int32) // top_count
    slot_token = (
        jnp.full((expert_count * tp_count * capacity,), -1, jnp.int32)
        .at[slot_of.reshape(-1)]
        .set(token_ids)
    )
    outgoing = jnp.where(
        (slot_token >= 0)[:, None], normed[jnp.maximum(slot_token, 0)], jnp.zeros((), jnp.bfloat16)
    )
    outgoing = outgoing.reshape(ep_count, local_experts, tp_count, capacity, width)
    arrived = lax.all_to_all(outgoing, "ep", split_axis=0, concat_axis=0, tiled=True)
    slot_rows = arrived.shape[3]
    inputs = arrived[:, 0].reshape(-1, width)
    hidden = jax.nn.silu(jnp.dot(inputs, expert_gate[0], preferred_element_type=jnp.float32))
    hidden = (hidden * jnp.dot(inputs, expert_up[0], preferred_element_type=jnp.float32)).astype(
        jnp.bfloat16
    )
    output = jnp.dot(hidden, expert_down[0], preferred_element_type=jnp.float32)
    results = [output.astype(jnp.bfloat16).reshape(ep_count, tp_count, slot_rows, width)]
    partial_value = jnp.stack(results, 1)
    shared_hidden = jax.nn.silu(jnp.dot(normed, shared_gate, preferred_element_type=jnp.float32))
    shared_hidden = (
        shared_hidden * jnp.dot(normed, shared_up, preferred_element_type=jnp.float32)
    ).astype(jnp.bfloat16)
    shared_part = jnp.dot(shared_hidden, shared_down, preferred_element_type=jnp.float32).astype(
        jnp.bfloat16
    )
    slot_total, shared_total = (
        lax.psum_scatter(
            partial_value.astype(jnp.float32).astype(jnp.bfloat16),
            "tp",
            scatter_dimension=2,
            tiled=True,
        ).astype(jnp.float32),
        lax.psum_scatter(
            shared_part.astype(jnp.float32)
            .reshape(1, 1, tp_count, MOE_DEV, width)
            .astype(jnp.bfloat16),
            "tp",
            scatter_dimension=2,
            tiled=True,
        ).astype(jnp.float32),
    )
    arrived_sums = lax.all_to_all(
        slot_total.astype(jnp.bfloat16), "ep", split_axis=0, concat_axis=0, tiled=True
    ).astype(slot_total.dtype)
    own_block = lax.axis_index("tp")
    own_entries = lax.dynamic_slice_in_dim(routes, own_block * MOE_DEV, MOE_DEV, 0)
    own_rank = lax.dynamic_slice_in_dim(
        rank_in.reshape(-1, top_count), own_block * MOE_DEV, MOE_DEV, 0
    )
    own_weight = lax.dynamic_slice_in_dim(route_weight, own_block * MOE_DEV, MOE_DEV, 0)
    picked = arrived_sums.reshape(-1, width)[own_entries * capacity + own_rank]
    moe_out = (
        jnp.sum(own_weight[..., None] * picked, 1) + shared_total.reshape(MOE_DEV, width)
    ).astype(jnp.bfloat16)
    return (mixed, moe_out)


LANES = 128
LOG2E = 1.4426950408889634
MESH = pl.DeviceIdType.MESH


class Refs:
    pass


def fused_kernel(names, *refs):
    r = Refs()
    for name, ref in zip(names, refs):
        setattr(r, name, ref)
    f32, bf16 = jnp.float32, jnp.bfloat16
    e = lax.axis_index("ep")
    t = lax.axis_index("tp")
    c = t % 2
    d = t // 2
    ex, ey = e % 2, e // 2
    partner = (e, t + 1 - 2 * c)
    rows = r.kv_hbm.shape[0]
    half = rows // 2
    tile = rows // 4
    eighth = rows // 8
    latent = r.kv_hbm.shape[1]
    heads = r.k_all.shape[0]
    width = r.moe_hbm.shape[1]
    slots = r.xs.shape[1] // 2
    side = r.nrm.shape[1]
    depths = side // MOE_DEV
    capacity = slots // depths
    factor = float(NOPE + ROPE_DIM) ** (-0.5) * LOG2E
    halfway = ROPE_DIM // 2

    def ep_of(k):
        return ((ey + k // 2) % 2) * 2 + (ex + k % 2) % 2

    def rel_of(source):
        return ((source // 2 + ey) % 2) * 2 + (source % 2 + ex) % 2

    def remote(src, dst, send, recv, device):
        return pltpu.make_async_remote_copy(
            src_ref=src, dst_ref=dst, send_sem=send, recv_sem=recv,
            device_id=device, device_id_type=MESH,
        )

    loads = {}

    def load(name, src, dst, sem):
        copy = pltpu.make_async_copy(src, dst, r.ld.at[sem])
        copy.start()
        loads[name] = copy

    load("kv", r.kv_hbm, r.kv_raw, 0)
    load("table", r.table_hbm.at[pl.ds(pl.multiple_of(e * tile, tile), tile)], r.table, 1)
    for q in range(2):
        for j in range(depths):
            start = (2 * j + (c + q) % 2) * MOE_DEV
            load(
                f"moe{q}{j}",
                r.moe_hbm.at[pl.ds(pl.multiple_of(start, MOE_DEV), MOE_DEV)],
                r.nrm.at[q, pl.ds(j * MOE_DEV, MOE_DEV)],
                2 + q * depths + j,
            )
    first = 2 + 2 * depths
    load("q", r.q_hbm, r.q_raw, first)
    load("sg", r.sg_hbm, r.sg, first + 1)
    load("su", r.su_hbm, r.su, first + 2)
    load("sd", r.sd_hbm, r.sd, first + 3)
    load("eg", r.eg_hbm.at[0], r.eg, first + 4)
    load("eu", r.eu_hbm.at[0], r.eu, first + 5)
    load("ed", r.ed_hbm.at[0], r.ed, first + 6)
    load("wo", r.wo_hbm, r.wo, first + 7)

    barrier = pltpu.get_barrier_semaphore()
    peers = [partner] + [(ep_of(k), t) for k in (1, 2, 3)]
    peers += [(e, ((d + j) % depths) * 2 + c) for j in range(1, depths)]
    for peer in peers:
        pl.semaphore_signal(barrier, inc=1, device_id=peer, device_id_type=MESH)

    lane = lax.broadcasted_iota(jnp.int32, (tile, LANES), 1)
    low = (lane >= NOPE) & (lane < NOPE + halfway)
    high = (lane >= NOPE + halfway) & (lane < NOPE + ROPE_DIM)

    def rotated(values, cosine, sine):
        swapped = jnp.where(
            lane < NOPE + halfway,
            pltpu.roll(values, LANES - halfway, 1),
            pltpu.roll(values, halfway, 1),
        )
        return values * cosine + swapped * sine

    loads["table"].wait()
    for i in range(4):
        turned = pltpu.roll(r.table[...], (NOPE - ROPE_DIM * i) % LANES, 1)
        later = pltpu.roll(turned, halfway, 1)
        sooner = pltpu.roll(turned, LANES - halfway, 1)
        here = pl.ds(i * tile, tile)
        r.cosine[here, :] = jnp.where(
            lane < NOPE, 1.0, jnp.where(low, turned, jnp.where(high, later, 0.0))
        )
        r.sine[here, :] = jnp.where(low, -sooner, jnp.where(high, turned, 0.0))

    place = (
        lax.broadcasted_iota(jnp.int32, (ROPE_DIM, LANES), 0) + NOPE
        == lax.broadcasted_iota(jnp.int32, (ROPE_DIM, LANES), 1)
    ).astype(f32).astype(bf16)

    loads["kv"].wait()
    packed = [jnp.zeros((eighth, LANES), f32) for _ in range(2)]
    for i in range(4):
        here = pl.ds(i * tile, tile)
        values = r.kv_raw[here, :].astype(f32)
        scale = lax.rsqrt(jnp.mean(values * values, -1, keepdims=True) + norm_eps)
        r.kvs[0, here, :] = (values * scale * r.kv_gain[...]).astype(bf16)
        straight = jnp.dot(r.rope[here, :], place, preferred_element_type=f32)
        turned = rotated(straight, r.cosine[here, :], r.sine[here, :])
        for part in range(2):
            g = 2 * (i % 2) + part
            piece = turned[part * eighth : (part + 1) * eighth]
            packed[i // 2] += pltpu.roll(piece, (ROPE_DIM * g - NOPE) % LANES, 1)
    for h in range(2):
        r.ropes[0, h] = packed[h].astype(bf16)

    pl.semaphore_wait(barrier, len(peers))

    own_half = pl.ds(pl.multiple_of(c * half, half), half)

    def pack_copies(k):
        device = (ep_of(k), t)
        return [
            remote(r.kvs.at[0, own_half], r.kvs.at[k, own_half],
                   r.pk_s.at[k - 1, 0], r.pk_r.at[k - 1, 0], device),
            remote(r.ropes.at[0, c], r.ropes.at[k, c],
                   r.pk_s.at[k - 1, 1], r.pk_r.at[k - 1, 1], device),
        ]

    def pack_forwards(k):
        return [
            remote(r.kvs.at[k, own_half], r.kvs.at[k, own_half],
                   r.pf_s.at[k - 1, 0], r.pf_r.at[k - 1, 0], partner),
            remote(r.ropes.at[k, c], r.ropes.at[k, c],
                   r.pf_s.at[k - 1, 1], r.pf_r.at[k - 1, 1], partner),
        ]

    for k in (3, 2, 1):

        @pl.when(ep_of(k) > e)
        def _(k=k):
            for copy in pack_copies(k):
                copy.start()

    for q in range(2):
        for j in range(depths):
            loads[f"moe{q}{j}"].wait()

    chunk = 16

    def norm_rows(i, _):
        q = i // (side // chunk)
        here = pl.ds(pl.multiple_of((i % (side // chunk)) * chunk, chunk), chunk)
        values = r.nrm[q, here, :].astype(f32)
        centred = values - jnp.mean(values, -1, keepdims=True)
        scale = lax.rsqrt(jnp.mean(centred * centred, -1, keepdims=True) + layer_eps)
        r.nrm[q, here, :] = (centred * scale * r.moe_gain[...]).astype(bf16)
        return 0

    lax.fori_loop(0, 2 * side // chunk, norm_rows, 0)

    row_id = lax.broadcasted_iota(jnp.int32, (side, side), 0)
    col_id = lax.broadcasted_iota(jnp.int32, (side, side), 1)
    earlier = (
        (col_id < row_id) & (col_id // MOE_DEV == row_id // MOE_DEV)
    ).astype(f32).astype(bf16)

    def gather_rows(ref, q):
        return jnp.concatenate(
            [
                ref[pl.ds(pl.multiple_of((2 * j + (c + q) % 2) * MOE_DEV, MOE_DEV), MOE_DEV), :]
                for j in range(depths)
            ],
            0,
        )

    lane_side = lax.broadcasted_iota(jnp.int32, (side, LANES), 1)
    block_of = lax.broadcasted_iota(jnp.int32, (side, LANES), 0) // MOE_DEV
    for q in range(2):
        routes = gather_rows(r.routes, q)
        named = lane_side < 0
        for k in range(routes.shape[1]):
            named = named | (routes[:, k : k + 1] == lane_side)
        marked = named.astype(f32)
        rank = jnp.dot(earlier, marked.astype(bf16), preferred_element_type=f32)
        slot = jnp.where(named, rank + (block_of * capacity).astype(f32), -1.0)
        for k in (3, 2, 1, 0) if q == 0 else (0,):
            target = ep_of(k)
            mine = jnp.sum(jnp.where(lane_side == target, slot, 0.0), -1, keepdims=True)
            onehot = (mine == lane_side.astype(f32)).astype(f32)
            if q == 0:
                r.onehot[k] = onehot.astype(bf16)
            picked = jnp.dot(
                onehot.T.astype(bf16), r.nrm[q], preferred_element_type=f32
            )[:slots].astype(bf16)
            if k == 0:
                r.xs[0, q * slots : (q + 1) * slots, :] = picked
            else:
                r.snd[k - 1] = picked
                slot_copy = remote(
                    r.snd.at[k - 1], r.xs.at[k, pl.ds(0, slots)],
                    r.sl_s.at[k - 1], r.sl_r.at[k - 1], (target, t),
                )
                slot_copy.start()

    def slot_sends(k):
        return remote(
            r.snd.at[k - 1], r.xs.at[k, pl.ds(0, slots)],
            r.sl_s.at[k - 1], r.sl_r.at[k - 1], (ep_of(k), t),
        )

    def slot_forward(k):
        return remote(
            r.xs.at[k, pl.ds(0, slots)], r.xs.at[k, pl.ds(slots, slots)],
            r.sf_s.at[k - 1], r.sf_r.at[k - 1], partner,
        )

    def silu(values):
        return values / (1.0 + jnp.exp(-values))

    for name in ("sg", "su", "sd"):
        loads[name].wait()
    for q in range(2):
        inputs = r.nrm[q]
        hidden = silu(jnp.dot(inputs, r.sg[...], preferred_element_type=f32))
        hidden = (hidden * jnp.dot(inputs, r.su[...], preferred_element_type=f32)).astype(bf16)
        r.shared[q] = jnp.dot(hidden, r.sd[...], preferred_element_type=f32).astype(bf16)
    shared_copy = remote(r.shared.at[1], r.shared.at[2], r.sh_s, r.sh_r, partner)
    shared_copy.start()

    loads["q"].wait()

    def project(i, _):
        here = pl.ds(pl.multiple_of(i * tile, tile), tile)
        values = r.q_raw[here, :].astype(f32)
        scale = lax.rsqrt(jnp.mean(values * values, -1, keepdims=True) + norm_eps)
        normed = (values * scale * r.q_gain[...]).astype(bf16)
        projected = jnp.dot(normed, r.wq[...], preferred_element_type=f32)
        for head in range(heads):
            straight = projected[:, head * LANES : (head + 1) * LANES]
            r.q_all[head, here, :] = rotated(
                straight, r.cosine[here, :], r.sine[here, :]
            ).astype(bf16)
        return 0

    lax.fori_loop(0, 4, project, 0)

    lane_half = lax.broadcasted_iota(jnp.int32, (half, LANES), 1)

    def expand(k):
        for h in range(2):
            source = r.ropes[k, h].astype(f32)
            pieces = [
                pltpu.roll(source, (NOPE - ROPE_DIM * g) % LANES, 1) for g in range(4)
            ]
            turned = jnp.concatenate(pieces, 0)
            turned = jnp.where(
                (lane_half >= NOPE) & (lane_half < NOPE + ROPE_DIM), turned, 0.0
            )
            product = jnp.dot(
                r.kvs[k, h * half : (h + 1) * half, :], r.wkv[...], preferred_element_type=f32
            )
            start = pl.ds(pl.multiple_of(k * rows + h * half, half), half)
            for head in range(heads):
                pair = product[:, head * LANES : (head + 1) * LANES]
                r.k_all[head, start, :] = jnp.where(lane_half < NOPE, pair, turned).astype(bf16)
                r.v_all[head, start, :] = jnp.where(lane_half == 0, 1.0, pair).astype(bf16)

    def attend(queries, carry, start, size, masked):
        scored = [
            lax.dot_general(
                queries[head],
                r.k_all[head, pl.ds(start, size), :],
                (((1,), (1,)), ((), ())),
                preferred_element_type=f32,
            )
            for head in range(heads)
        ]
        result = []
        for head in range(heads):
            scores = scored[head]
            old_max, acc = carry[head]
            if masked:
                row = lax.broadcasted_iota(jnp.int32, scores.shape, 0)
                column = lax.broadcasted_iota(jnp.int32, scores.shape, 1)
                scores = jnp.where(column <= row, scores, -jnp.inf)
            new_max = jnp.maximum(old_max, jnp.max(scores, -1, keepdims=True))
            weights = jnp.exp2((scores - new_max) * factor).astype(bf16)
            product = jnp.dot(
                weights, r.v_all[head, pl.ds(start, size), :], preferred_element_type=f32
            )
            result.append((new_max, acc * jnp.exp2((old_max - new_max) * factor) + product))
        return tuple(result)

    expand(0)

    def local_tile(i, _):
        here = pl.ds(pl.multiple_of(i * tile, tile), tile)
        queries = [r.q_all[head, here, :] for head in range(heads)]
        carry = tuple(
            (jnp.full((tile, 1), floor_value, f32), jnp.zeros((tile, LANES), f32))
            for head in range(heads)
        )
        carry = attend(queries, carry, pl.multiple_of(i * tile, tile), tile, True)
        carry = lax.fori_loop(
            0, i,
            lambda j, cc: attend(queries, cc, pl.multiple_of(j * tile, tile), tile, False),
            carry,
        )
        for head in range(heads):
            r.top[head, here, :] = jnp.broadcast_to(carry[head][0], (tile, LANES))
            r.acc[head, here, :] = carry[head][1]
        return 0

    lax.fori_loop(0, 4, local_tile, 0)

    for k in (1, 2, 3):

        @pl.when(ep_of(k) < e)
        def _(k=k):
            for copy, forward in zip(pack_copies(k), pack_forwards(k)):
                copy.wait_recv()
                forward.start()

    for k in (1, 2, 3):

        @pl.when(ep_of(k) < e)
        def _(k=k):
            for forward in pack_forwards(k):
                forward.wait_recv()
            expand(k)

    head_cols = heads * VDIM
    own_cols = pl.ds(pl.multiple_of(t * head_cols, head_cols), head_cols)

    def remote_tile(i, _):
        here = pl.ds(pl.multiple_of(i * tile, tile), tile)
        queries = [r.q_all[head, here, :] for head in range(heads)]
        carry = tuple(
            (r.top[head, here, :][:, :1], r.acc[head, here, :]) for head in range(heads)
        )
        carry = lax.fori_loop(
            0, e,
            lambda s, cc: attend(
                queries, cc, pl.multiple_of(rel_of(s) * rows, rows), rows, False
            ),
            carry,
        )
        outs = [acc[:, NOPE : NOPE + VDIM] / acc[:, :1] for _, acc in carry]
        r.mixers[here, own_cols] = jnp.concatenate(outs, -1).astype(bf16)
        return 0

    lax.fori_loop(0, 4, remote_tile, 0)

    def depth_of(j):
        return (d + j) % depths

    def head_copy(j):
        device = partner if j == 0 else (e, depth_of(j) * 2 + c)
        return remote(
            r.mixers.at[:, own_cols], r.mixers.at[:, own_cols],
            r.h_s.at[j], r.h_r.at[j], device,
        )

    def head_forward(j):
        source = ((d + depths - j) % depths) * 2 + c
        cols = pl.ds(pl.multiple_of(source * head_cols, head_cols), head_cols)
        return remote(
            r.mixers.at[:, cols], r.mixers.at[:, cols],
            r.hf_s.at[j - 1], r.hf_r.at[j - 1], partner,
        )

    for j in range(depths):
        head_copy(j).start()

    for k in (3, 2, 1):
        slot_sends(k).wait_recv()
        slot_forward(k).start()
    for name in ("eg", "eu", "ed"):
        loads[name].wait()

    def partial_copy(k):
        return remote(r.theirs.at[k], r.pair.at[k], r.ex_s.at[k], r.ex_r.at[k], partner)

    def return_copy(k):
        return remote(
            r.sums.at[k], r.back.at[k, pl.ds(0, slots)],
            r.rt_s.at[k - 1], r.rt_r.at[k - 1], (ep_of(k), t),
        )

    hidden_units = r.eg.shape[1]
    step = min(256, hidden_units)
    out_step = min(512, width)

    def run_expert(k):
        inputs = r.xs[k]
        hidden = []
        for n in range(0, hidden_units, step):
            gate = silu(jnp.dot(inputs, r.eg[:, n : n + step], preferred_element_type=f32))
            up = jnp.dot(inputs, r.eu[:, n : n + step], preferred_element_type=f32)
            hidden.append((gate * up).astype(bf16))
        hidden = jnp.concatenate(hidden, 1)
        for n in range(0, width, out_step):
            product = jnp.dot(
                hidden, r.ed[:, n : n + out_step], preferred_element_type=f32
            ).astype(bf16)
            r.ours[k, :, n : n + out_step] = product[:slots]
            r.theirs[k, :, n : n + out_step] = product[slots:]
        partial_copy(k).start()

    def sum_pair(k):
        partial_copy(k).wait_recv()
        return (r.ours[k].astype(f32) + r.pair[k].astype(f32)).astype(bf16)

    def routed(i, _):
        k = 3 - i
        slot_forward(k).wait_recv()
        run_expert(k)

        @pl.when(i > 0)
        def _():
            r.sums[k + 1] = sum_pair(k + 1)
            return_copy(k + 1).start()

        return 0

    r.back[:, slots:, :] = jnp.zeros((4, r.back.shape[1] - slots, width), bf16)
    lax.fori_loop(0, 3, routed, 0)
    run_expert(0)
    r.sums[1] = sum_pair(1)
    return_copy(1).start()
    r.back[0, :slots, :] = sum_pair(0)
    shared_copy.wait_recv()

    for k in (3, 2, 1):
        return_copy(k).wait_recv()
    routes = gather_rows(r.routes, 0)
    weight = gather_rows(r.route_weight, 0)
    factors = [
        jnp.sum(jnp.where(routes == ep_of(k), weight, 0.0), -1, keepdims=True) for k in range(4)
    ]
    for n in range(0, width, out_step):
        cols = slice(n, n + out_step)
        total = r.shared[0, :, cols].astype(f32) + r.shared[2, :, cols].astype(f32)
        for k in range(4):
            total = total + factors[k] * jnp.dot(
                r.onehot[k], r.back[k, :, cols], preferred_element_type=f32
            )
        r.zs[:, cols] = total.astype(bf16)

    def z_copy(j):
        there = depth_of(j)
        return remote(
            r.zs.at[pl.ds(pl.multiple_of(there * MOE_DEV, MOE_DEV), MOE_DEV)],
            r.zr.at[j - 1],
            r.z_s.at[j - 1], r.z_r.at[j - 1], (e, there * 2 + c),
        )

    for j in range(1, depths):
        z_copy(j).start()

    for j in range(1, depths):
        head_copy(j).wait_recv()
        head_forward(j).start()
    loads["wo"].wait()
    head_copy(0).wait_recv()
    for j in range(1, depths):
        head_forward(j).wait_recv()

    def mix(i, _):
        here = pl.ds(pl.multiple_of(i * tile, tile), tile)
        r.mixed[here, :] = jnp.dot(
            r.mixers[here, :], r.wo[...], preferred_element_type=f32
        ).astype(bf16)
        return 0

    lax.fori_loop(0, 4, mix, 0)

    final = r.zs[pl.ds(pl.multiple_of(d * MOE_DEV, MOE_DEV), MOE_DEV), :].astype(f32)
    for j in range(1, depths):
        z_copy(j).wait_recv()
        final = final + r.zr[j - 1].astype(f32)
    r.moe_out[...] = final.astype(bf16)

    for k in (1, 2, 3):

        @pl.when(ep_of(k) > e)
        def _(k=k):
            for copy in pack_copies(k):
                copy.wait_send()

        @pl.when(ep_of(k) < e)
        def _(k=k):
            for copy in pack_forwards(k):
                copy.wait_send()

        slot_sends(k).wait_send()
        slot_forward(k).wait_send()
        return_copy(k).wait_send()
    shared_copy.wait_send()
    for k in range(4):
        partial_copy(k).wait_send()
    head_copy(0).wait_send()
    for j in range(1, depths):
        head_copy(j).wait_send()
        head_forward(j).wait_send()
        z_copy(j).wait_send()


def rotary_constant(total, per_device):
    halfway = ROPE_DIM // 2
    inverse = (
        np.float32(rotary_base)
        ** (-(np.arange(halfway, dtype=np.float32) * np.float32(2.0) / np.float32(ROPE_DIM)))
    ).astype(np.float32)
    angles = (np.arange(total, dtype=np.float32)[:, None] * inverse[None, :]).astype(np.float32)
    angles = angles.astype(np.float64)
    both = np.concatenate([np.cos(angles), np.sin(angles)], 1).astype(np.float32)
    groups = both.reshape(-1, LANES // ROPE_DIM, per_device * ROPE_DIM // LANES, ROPE_DIM)
    return groups.transpose(0, 2, 1, 3).reshape(-1, LANES)


def fused_body(
    q_latent,
    kv_latent,
    rope_key,
    q_gain,
    kv_gain,
    w_query,
    w_keyval,
    w_output,
    moe_input,
    moe_gain,
    routes,
    route_weight,
    expert_gate,
    expert_up,
    expert_down,
    shared_gate,
    shared_up,
    shared_down,
):
    rows, qlat = q_latent.shape
    latent = kv_latent.shape[1]
    ep_count = lax.axis_size("ep")
    tp_count = lax.axis_size("tp")
    heads = w_query.shape[1] // (NOPE + ROPE_DIM)
    tokens, width = moe_input.shape
    side = tokens // 2
    depths = tp_count // 2
    hidden = expert_gate.shape[2]
    shared_hidden = shared_gate.shape[1]
    top = routes.shape[1]
    capacity = 3 * MOE_DEV * top // (2 * ep_count)
    slots = depths * capacity
    columns = w_output.shape[1]
    bf16, f32 = jnp.bfloat16, jnp.float32
    table = jnp.asarray(rotary_constant(rows * ep_count, rows))
    padded = jnp.pad(
        w_query.reshape(qlat, heads, NOPE + ROPE_DIM),
        ((0, 0), (0, 0), (0, LANES - NOPE - ROPE_DIM)),
    ).reshape(qlat, heads * LANES)
    hbm = pl.BlockSpec(memory_space=pltpu.HBM)
    vmem = pl.BlockSpec(memory_space=pltpu.VMEM)
    inputs = [
        ("q_hbm", q_latent, hbm),
        ("kv_hbm", kv_latent, hbm),
        ("table_hbm", table, hbm),
        ("moe_hbm", moe_input, hbm),
        ("eg_hbm", expert_gate, hbm),
        ("eu_hbm", expert_up, hbm),
        ("ed_hbm", expert_down, hbm),
        ("sg_hbm", shared_gate, hbm),
        ("su_hbm", shared_up, hbm),
        ("sd_hbm", shared_down, hbm),
        ("wo_hbm", w_output, hbm),
        ("rope", rope_key, vmem),
        ("q_gain", q_gain.reshape(1, -1), vmem),
        ("kv_gain", kv_gain.reshape(1, -1), vmem),
        ("wq", padded, vmem),
        ("wkv", w_keyval, vmem),
        ("moe_gain", moe_gain.reshape(1, -1), vmem),
        ("routes", routes, vmem),
        ("route_weight", route_weight, vmem),
    ]
    outputs = [("mixed", (rows, columns)), ("moe_out", (MOE_DEV, width))]
    dma = pltpu.SemaphoreType.DMA
    scratch = [
        ("kv_raw", pltpu.VMEM((rows, latent), bf16)),
        ("q_raw", pltpu.VMEM((rows, qlat), bf16)),
        ("table", pltpu.VMEM((rows // 4, LANES), f32)),
        ("cosine", pltpu.VMEM((rows, LANES), f32)),
        ("sine", pltpu.VMEM((rows, LANES), f32)),
        ("kvs", pltpu.VMEM((4, rows, latent), bf16)),
        ("ropes", pltpu.VMEM((4, 2, rows // 8, LANES), bf16)),
        ("nrm", pltpu.VMEM((2, side, width), bf16)),
        ("onehot", pltpu.VMEM((4, side, LANES), bf16)),
        ("snd", pltpu.VMEM((3, slots, width), bf16)),
        ("xs", pltpu.VMEM((4, 2 * slots, width), bf16)),
        ("shared", pltpu.VMEM((3, side, width), bf16)),
        ("q_all", pltpu.VMEM((heads, rows, LANES), bf16)),
        ("k_all", pltpu.VMEM((heads, 4 * rows, LANES), bf16)),
        ("v_all", pltpu.VMEM((heads, 4 * rows, LANES), bf16)),
        ("top", pltpu.VMEM((heads, rows, LANES), f32)),
        ("acc", pltpu.VMEM((heads, rows, LANES), f32)),
        ("mixers", pltpu.VMEM((rows, tp_count * heads * VDIM), bf16)),
        ("ours", pltpu.VMEM((4, slots, width), bf16)),
        ("theirs", pltpu.VMEM((4, slots, width), bf16)),
        ("pair", pltpu.VMEM((4, slots, width), bf16)),
        ("sums", pltpu.VMEM((4, slots, width), bf16)),
        ("back", pltpu.VMEM((4, LANES, width), bf16)),
        ("zs", pltpu.VMEM((side, width), bf16)),
        ("zr", pltpu.VMEM((depths - 1, MOE_DEV, width), bf16)),
        ("eg", pltpu.VMEM((width, hidden), bf16)),
        ("eu", pltpu.VMEM((width, hidden), bf16)),
        ("ed", pltpu.VMEM((hidden, width), bf16)),
        ("sg", pltpu.VMEM((width, shared_hidden), bf16)),
        ("su", pltpu.VMEM((width, shared_hidden), bf16)),
        ("sd", pltpu.VMEM((shared_hidden, width), bf16)),
        ("wo", pltpu.VMEM(w_output.shape, bf16)),
        ("ld", dma((10 + 2 * depths,))),
        ("pk_s", dma((3, 2))),
        ("pk_r", dma((3, 2))),
        ("pf_s", dma((3, 2))),
        ("pf_r", dma((3, 2))),
        ("sl_s", dma((3,))),
        ("sl_r", dma((3,))),
        ("sf_s", dma((3,))),
        ("sf_r", dma((3,))),
        ("sh_s", dma),
        ("sh_r", dma),
        ("ex_s", dma((4,))),
        ("ex_r", dma((4,))),
        ("rt_s", dma((3,))),
        ("rt_r", dma((3,))),
        ("h_s", dma((depths,))),
        ("h_r", dma((depths,))),
        ("hf_s", dma((depths - 1,))),
        ("hf_r", dma((depths - 1,))),
        ("z_s", dma((depths - 1,))),
        ("z_r", dma((depths - 1,))),
    ]
    names = [x[0] for x in inputs] + [x[0] for x in outputs] + [x[0] for x in scratch]
    mixed, moe_out = pl.pallas_call(
        lambda *refs: fused_kernel(names, *refs),
        out_shape=[jax.ShapeDtypeStruct(shape, bf16) for _, shape in outputs],
        in_specs=[spec for _, _, spec in inputs],
        out_specs=[vmem] * len(outputs),
        scratch_shapes=[spec for _, spec in scratch],
        compiler_params=pltpu.CompilerParams(
            collective_id=0,
            has_side_effects=True,
            vmem_limit_bytes=60 * 1024 * 1024,
        ),
        name="fused",
    )(*[value for _, value, _ in inputs])
    return (mixed, moe_out)


def solution(mesh):
    in_specs = (
        P("ep", None),
        P("ep", None),
        P("ep", None),
        P(),
        P(),
        P(None, "tp"),
        P(None, "tp"),
        P(None, "tp"),
        P("ep", None),
        P(),
        P("ep", None),
        P("ep", None),
        P("ep", None, "tp"),
        P("ep", None, "tp"),
        P("ep", "tp", None),
        P(None, "tp"),
        P(None, "tp"),
        P("tp", None),
    )
    out_specs = (P("ep", "tp"), P(("ep", "tp"), None))
    chosen = fused_body if mesh.shape["ep"] == 4 else body
    return jax.shard_map(
        chosen, mesh=mesh, in_specs=in_specs, out_specs=out_specs, check_vma=False
    )
```

```python
import jax
import jax.numpy as jnp
import numpy as np
from jax import lax
from jax.experimental import pallas as pl
from jax.experimental.pallas import tpu as pltpu
from jax.sharding import PartitionSpec as P

NOPE = 64
ROPE_DIM = 32
VDIM = 64
MOE_DEV = 32


norm_eps = 1e-06
layer_eps = 1e-05
rotary_base = 10000.0
floor_value = -1e30


def rms_scale(values, gain):
    widened = values.astype(jnp.float32)
    return (
        widened * lax.rsqrt(jnp.mean(widened * widened, -1, keepdims=True) + norm_eps) * gain
    ).astype(jnp.bfloat16)


def layer_scale(values, gain):
    widened = values.astype(jnp.float32)
    centred = widened - jnp.mean(widened, -1, keepdims=True)
    return (
        centred * lax.rsqrt(jnp.mean(centred * centred, -1, keepdims=True) + layer_eps) * gain
    ).astype(jnp.bfloat16)


def rotary_tables(positions):
    halfway = ROPE_DIM // 2
    inverse = rotary_base ** (-(jnp.arange(halfway, dtype=jnp.float32) * 2.0 / ROPE_DIM))
    angles = positions.astype(jnp.float32)[:, None] * inverse[None, :]
    return (jnp.cos(angles), jnp.sin(angles))


def rotate(values, cosine_table, sine_table):
    halfway = values.shape[-1] // 2
    first_half = values[..., :halfway]
    second_half = values[..., halfway:]
    return jnp.concatenate(
        [
            first_half * cosine_table - second_half * sine_table,
            second_half * cosine_table + first_half * sine_table,
        ],
        -1,
    )


def block_stats(query_block, query_pos, keyvals, rotated_keys, key_pos):
    scale = float(NOPE + ROPE_DIM) ** (-0.5)
    scores = jnp.einsum(
        "qhd,khd->hqk",
        query_block[..., :NOPE],
        keyvals[..., :NOPE],
        preferred_element_type=jnp.float32,
    )
    scores = (
        scores
        + jnp.einsum(
            "qhd,kd->hqk", query_block[..., NOPE:], rotated_keys, preferred_element_type=jnp.float32
        )
    ) * scale
    allowed = key_pos[None, :] <= query_pos[:, None]
    scores = jnp.where(allowed[None], scores, -jnp.inf)
    block_max = jnp.max(scores, -1)
    weights = jnp.exp(scores - block_max[..., None])
    block_sum = jnp.sum(weights, -1)
    attended = jnp.einsum(
        "hqk,khd->qhd",
        weights.astype(jnp.bfloat16),
        keyvals[..., NOPE:],
        preferred_element_type=jnp.float32,
    ).astype(jnp.bfloat16)
    return (block_max.T, block_sum.T, attended)


def merge_block(carried, stats):
    running_max, running_sum, running_acc = carried
    block_max, block_sum, attended = stats
    new_max = jnp.maximum(running_max, block_max)
    old_weight = jnp.exp(running_max - new_max)
    new_weight = jnp.exp(block_max - new_max)
    return (
        new_max,
        running_sum * old_weight + block_sum * new_weight,
        running_acc * old_weight[..., None] + attended.astype(jnp.float32) * new_weight[..., None],
    )


def body(
    q_latent,
    kv_latent,
    rope_key,
    q_gain,
    kv_gain,
    w_query,
    w_keyval,
    w_output,
    moe_input,
    moe_gain,
    routes,
    route_weight,
    expert_gate,
    expert_up,
    expert_down,
    shared_gate,
    shared_up,
    shared_down,
):
    row_count = q_latent.shape[0]
    own_index = lax.axis_index("ep")
    ep_count = lax.axis_size("ep")
    tp_count = lax.axis_size("tp")
    positions = own_index * row_count + jnp.arange(row_count, dtype=jnp.int32)
    cosine_table, sine_table = rotary_tables(positions)
    q_normed = rms_scale(q_latent, q_gain)
    kv_normed = rms_scale(kv_latent, kv_gain)
    key_rotated = rotate(rope_key.astype(jnp.float32), cosine_table, sine_table).astype(
        jnp.bfloat16
    )
    heads_local = w_query.shape[1] // (NOPE + ROPE_DIM)
    projected = jnp.dot(q_normed, w_query, preferred_element_type=jnp.float32)
    projected = projected.reshape(row_count, heads_local, NOPE + ROPE_DIM)
    queries = jnp.concatenate(
        [
            projected[..., :NOPE],
            rotate(projected[..., NOPE:], cosine_table[:, None, :], sine_table[:, None, :]),
        ],
        -1,
    ).astype(jnp.bfloat16)

    def expand_keys(latent_rows):
        expanded = jnp.dot(latent_rows, w_keyval, preferred_element_type=jnp.float32).astype(
            jnp.bfloat16
        )
        return expanded.reshape(latent_rows.shape[0], heads_local, NOPE + VDIM)

    initial = (
        jnp.full((row_count, heads_local), floor_value, jnp.float32),
        jnp.zeros((row_count, heads_local), jnp.float32),
        jnp.zeros((row_count, heads_local, VDIM), jnp.float32),
    )
    carried = initial
    latent_piece = lax.all_gather(kv_normed, "ep", axis=0, tiled=True)
    rotated_piece = lax.all_gather(key_rotated, "ep", axis=0, tiled=True)
    block_count = latent_piece.shape[0] // row_count

    def visit_block(inner, offset):

        def live(current):
            latent_rows = lax.dynamic_slice_in_dim(latent_piece, offset * row_count, row_count, 0)
            rotated_rows = lax.dynamic_slice_in_dim(rotated_piece, offset * row_count, row_count, 0)
            key_pos = offset * row_count + jnp.arange(row_count, dtype=jnp.int32)
            stats = block_stats(queries, positions, expand_keys(latent_rows), rotated_rows, key_pos)
            return merge_block(current, stats)

        def skipped(current):
            return current

        return (lax.cond(offset <= own_index, live, skipped, inner), None)

    carried, unused = lax.scan(visit_block, carried, jnp.arange(block_count, dtype=jnp.int32))
    running_max, running_sum, running_acc = carried
    heads_out = (
        (running_acc / running_sum[..., None])
        .astype(jnp.bfloat16)
        .reshape(row_count, heads_local * VDIM)
    )
    mixed = jnp.dot(
        lax.all_gather(heads_out, "tp", axis=1, tiled=True),
        w_output,
        preferred_element_type=jnp.float32,
    )
    mixed = mixed.astype(jnp.bfloat16)
    width = moe_input.shape[1]
    top_count = routes.shape[1]
    local_experts = expert_gate.shape[0]
    expert_count = local_experts * ep_count
    capacity = max(2, 3 * MOE_DEV * top_count // (2 * expert_count))
    normed = layer_scale(moe_input, moe_gain)
    entries = routes.reshape(tp_count, MOE_DEV * top_count)
    onehot = (entries[..., None] == jnp.arange(expert_count, dtype=jnp.int32)).astype(jnp.int32)
    earlier = jnp.cumsum(onehot, 1) - onehot
    rank_in = jnp.sum(earlier * onehot, -1)
    block_ids = jnp.arange(tp_count, dtype=jnp.int32)[:, None]
    slot_of = ((entries * tp_count + block_ids) * capacity + rank_in).reshape(-1, top_count)
    token_ids = jnp.arange(tp_count * MOE_DEV * top_count, dtype=jnp.int32) // top_count
    slot_token = (
        jnp.full((expert_count * tp_count * capacity,), -1, jnp.int32)
        .at[slot_of.reshape(-1)]
        .set(token_ids)
    )
    outgoing = jnp.where(
        (slot_token >= 0)[:, None], normed[jnp.maximum(slot_token, 0)], jnp.zeros((), jnp.bfloat16)
    )
    outgoing = outgoing.reshape(ep_count, local_experts, tp_count, capacity, width)
    arrived = lax.all_to_all(outgoing, "ep", split_axis=0, concat_axis=0, tiled=True)
    slot_rows = arrived.shape[3]
    inputs = arrived[:, 0].reshape(-1, width)
    hidden = jax.nn.silu(jnp.dot(inputs, expert_gate[0], preferred_element_type=jnp.float32))
    hidden = (hidden * jnp.dot(inputs, expert_up[0], preferred_element_type=jnp.float32)).astype(
        jnp.bfloat16
    )
    output = jnp.dot(hidden, expert_down[0], preferred_element_type=jnp.float32)
    results = [output.astype(jnp.bfloat16).reshape(ep_count, tp_count, slot_rows, width)]
    partial_value = jnp.stack(results, 1)
    shared_hidden = jax.nn.silu(jnp.dot(normed, shared_gate, preferred_element_type=jnp.float32))
    shared_hidden = (
        shared_hidden * jnp.dot(normed, shared_up, preferred_element_type=jnp.float32)
    ).astype(jnp.bfloat16)
    shared_part = jnp.dot(shared_hidden, shared_down, preferred_element_type=jnp.float32).astype(
        jnp.bfloat16
    )
    slot_total, shared_total = (
        lax.psum_scatter(
            partial_value.astype(jnp.float32).astype(jnp.bfloat16),
            "tp",
            scatter_dimension=2,
            tiled=True,
        ).astype(jnp.float32),
        lax.psum_scatter(
            shared_part.astype(jnp.float32)
            .reshape(1, 1, tp_count, MOE_DEV, width)
            .astype(jnp.bfloat16),
            "tp",
            scatter_dimension=2,
            tiled=True,
        ).astype(jnp.float32),
    )
    arrived_sums = lax.all_to_all(
        slot_total.astype(jnp.bfloat16), "ep", split_axis=0, concat_axis=0, tiled=True
    ).astype(slot_total.dtype)
    own_block = lax.axis_index("tp")
    own_entries = lax.dynamic_slice_in_dim(routes, own_block * MOE_DEV, MOE_DEV, 0)
    own_rank = lax.dynamic_slice_in_dim(
        rank_in.reshape(-1, top_count), own_block * MOE_DEV, MOE_DEV, 0
    )
    own_weight = lax.dynamic_slice_in_dim(route_weight, own_block * MOE_DEV, MOE_DEV, 0)
    picked = arrived_sums.reshape(-1, width)[own_entries * capacity + own_rank]
    moe_out = (
        jnp.sum(own_weight[..., None] * picked, 1) + shared_total.reshape(MOE_DEV, width)
    ).astype(jnp.bfloat16)
    return (mixed, moe_out)


LANES = 128
LOG2E = 1.4426950408889634
MESH = pl.DeviceIdType.MESH


class Refs:
    pass


def fused_kernel(names, *refs):
    r = Refs()
    for name, ref in zip(names, refs):
        setattr(r, name, ref)
    f32, bf16 = jnp.float32, jnp.bfloat16
    e = lax.axis_index("ep")
    t = lax.axis_index("tp")
    c = t % 2
    d = t // 2
    ex, ey = e % 2, e // 2
    partner = (e, t + 1 - 2 * c)
    rows = r.kv_hbm.shape[0]
    half = rows // 2
    tile = rows // 4
    eighth = rows // 8
    latent = r.kv_hbm.shape[1]
    heads = r.k_all.shape[0]
    width = r.moe_hbm.shape[1]
    slots = r.xs.shape[1] // 2
    side = r.nrm.shape[1]
    depths = side // MOE_DEV
    capacity = slots // depths
    factor = float(NOPE + ROPE_DIM) ** (-0.5) * LOG2E
    halfway = ROPE_DIM // 2

    def ep_of(k):
        return ((ey + k // 2) % 2) * 2 + (ex + k % 2) % 2

    def rel_of(source):
        return ((source // 2 + ey) % 2) * 2 + (source % 2 + ex) % 2

    def remote(src, dst, send, recv, device):
        return pltpu.make_async_remote_copy(
            src_ref=src, dst_ref=dst, send_sem=send, recv_sem=recv,
            device_id=device, device_id_type=MESH,
        )

    loads = {}

    def load(name, src, dst, sem):
        copy = pltpu.make_async_copy(src, dst, r.ld.at[sem])
        copy.start()
        loads[name] = copy

    load("kv", r.kv_hbm, r.kv_raw, 0)
    load("table", r.table_hbm.at[pl.ds(pl.multiple_of(e * tile, tile), tile)], r.table, 1)
    for j in range(depths):
        load(
            f"moe{j}",
            r.moe_hbm.at[pl.ds(pl.multiple_of((2 * j + c) * MOE_DEV, MOE_DEV), MOE_DEV)],
            r.nrm.at[0, pl.ds(j * MOE_DEV, MOE_DEV)],
            2 + j,
        )
    first = 2 + depths
    load("q", r.q_hbm, r.q_raw, first)
    load("sg", r.sg_hbm, r.sg, first + 1)
    load("su", r.su_hbm, r.su, first + 2)
    load("sd", r.sd_hbm, r.sd, first + 3)
    load("eg", r.eg_hbm.at[0], r.eg, first + 4)
    load("eu", r.eu_hbm.at[0], r.eu, first + 5)
    load("ed", r.ed_hbm.at[0], r.ed, first + 6)
    load("wo", r.wo_hbm, r.wo, first + 7)

    barrier = pltpu.get_barrier_semaphore()
    peers = [partner] + [(ep_of(k), t) for k in (1, 2, 3)]
    peers += [(e, ((d + j) % depths) * 2 + c) for j in range(1, depths)]
    for peer in peers:
        pl.semaphore_signal(barrier, inc=1, device_id=peer, device_id_type=MESH)

    lane = lax.broadcasted_iota(jnp.int32, (tile, LANES), 1)
    low = (lane >= NOPE) & (lane < NOPE + halfway)
    high = (lane >= NOPE + halfway) & (lane < NOPE + ROPE_DIM)

    def rotated(values, cosine, sine):
        swapped = jnp.where(
            lane < NOPE + halfway,
            pltpu.roll(values, LANES - halfway, 1),
            pltpu.roll(values, halfway, 1),
        )
        return values * cosine + swapped * sine

    loads["table"].wait()
    for i in range(4):
        turned = pltpu.roll(r.table[...], (NOPE - ROPE_DIM * i) % LANES, 1)
        later = pltpu.roll(turned, halfway, 1)
        sooner = pltpu.roll(turned, LANES - halfway, 1)
        here = pl.ds(i * tile, tile)
        r.cosine[here, :] = jnp.where(
            lane < NOPE, 1.0, jnp.where(low, turned, jnp.where(high, later, 0.0))
        )
        r.sine[here, :] = jnp.where(low, -sooner, jnp.where(high, turned, 0.0))

    r.tags[...] = jnp.zeros(r.tags.shape, f32)
    top = r.routes_t.shape[0]
    r.tags[:top, :] = r.routes_t[...].astype(f32)
    r.tags[top : 2 * top, :] = r.weight_t[...]
    r.tagged[...] = r.tags[...].T

    place = (
        lax.broadcasted_iota(jnp.int32, (ROPE_DIM, LANES), 0) + NOPE
        == lax.broadcasted_iota(jnp.int32, (ROPE_DIM, LANES), 1)
    ).astype(f32).astype(bf16)

    loads["kv"].wait()
    packed = [jnp.zeros((eighth, LANES), f32) for _ in range(2)]
    for i in range(4):
        here = pl.ds(i * tile, tile)
        values = r.kv_raw[here, :].astype(f32)
        scale = lax.rsqrt(jnp.mean(values * values, -1, keepdims=True) + norm_eps)
        r.kvs[0, here, :] = (values * scale * r.kv_gain[...]).astype(bf16)
        straight = lax.dot_general(
            r.rope_t[:, i * tile : (i + 1) * tile], place,
            (((0,), (0,)), ((), ())), preferred_element_type=f32,
        )
        turned = rotated(straight, r.cosine[here, :], r.sine[here, :])
        for part in range(2):
            g = 2 * (i % 2) + part
            piece = turned[part * eighth : (part + 1) * eighth]
            packed[i // 2] += pltpu.roll(piece, (ROPE_DIM * g - NOPE) % LANES, 1)
    for h in range(2):
        r.ropes[0, h] = packed[h].astype(bf16)

    pl.semaphore_wait(barrier, len(peers))

    own_half = pl.ds(pl.multiple_of(c * half, half), half)

    def pack_copies(k):
        device = (ep_of(k), t)
        return [
            remote(r.kvs.at[0, own_half], r.kvs.at[k, own_half],
                   r.pk_s.at[k - 1, 0], r.pk_r.at[k - 1, 0], device),
            remote(r.ropes.at[0, c], r.ropes.at[k, c],
                   r.pk_s.at[k - 1, 1], r.pk_r.at[k - 1, 1], device),
        ]

    def pack_forwards(k):
        return [
            remote(r.kvs.at[k, own_half], r.kvs.at[k, own_half],
                   r.pf_s.at[k - 1, 0], r.pf_r.at[k - 1, 0], partner),
            remote(r.ropes.at[k, c], r.ropes.at[k, c],
                   r.pf_s.at[k - 1, 1], r.pf_r.at[k - 1, 1], partner),
        ]

    for k in (3, 2, 1):

        @pl.when(ep_of(k) > e)
        def _(k=k):
            for copy in pack_copies(k):
                copy.start()

    for j in range(depths):
        loads[f"moe{j}"].wait()

    chunk = 16

    def norm_rows(i, _):
        here = pl.ds(pl.multiple_of(i * chunk, chunk), chunk)
        values = r.nrm[0, here, :].astype(f32)
        centred = values - jnp.mean(values, -1, keepdims=True)
        scale = lax.rsqrt(jnp.mean(centred * centred, -1, keepdims=True) + layer_eps)
        r.nrm[0, here, :] = (centred * scale * r.moe_gain[...]).astype(bf16)
        return 0

    lax.fori_loop(0, side // chunk, norm_rows, 0, unroll=2)
    rows_copy = remote(r.nrm.at[0], r.nrm.at[1], r.rc_s, r.rc_r, partner)
    rows_copy.start()

    row_id = lax.broadcasted_iota(jnp.int32, (side, side), 0)
    col_id = lax.broadcasted_iota(jnp.int32, (side, side), 1)
    earlier = (
        (col_id < row_id) & (col_id // MOE_DEV == row_id // MOE_DEV)
    ).astype(f32).astype(bf16)

    def gather_rows(q):
        return jnp.concatenate(
            [
                r.tagged[pl.ds(pl.multiple_of((2 * j + (c + q) % 2) * MOE_DEV, MOE_DEV), MOE_DEV), :]
                for j in range(depths)
            ],
            0,
        )

    lane_side = lax.broadcasted_iota(jnp.int32, (side, LANES), 1)
    block_of = lax.broadcasted_iota(jnp.int32, (side, LANES), 0) // MOE_DEV
    def slot_sends(k):
        return remote(
            r.snd.at[k - 1], r.xs.at[k, pl.ds(0, slots)],
            r.sl_s.at[k - 1], r.sl_r.at[k - 1], (ep_of(k), t),
        )

    def slot_table(q):
        tags = gather_rows(q)
        named = lane_side < 0
        for k in range(top):
            named = named | (tags[:, k : k + 1] == lane_side.astype(f32))
        rank = jnp.dot(
            earlier, named.astype(f32).astype(bf16), preferred_element_type=f32
        )
        return jnp.where(named, rank + (block_of * capacity).astype(f32), -1.0)

    def pick_rows(slot, q, k):
        mine = jnp.sum(jnp.where(lane_side == ep_of(k), slot, 0.0), -1, keepdims=True)
        onehot = (mine == lane_side.astype(f32)).astype(f32)
        if q == 0:
            r.onehot[k] = onehot.astype(bf16)
        return jnp.dot(
            onehot.T.astype(bf16), r.nrm[q], preferred_element_type=f32
        )[:slots].astype(bf16)

    table = slot_table(0)
    for k in (3, 2, 1):
        r.snd[k - 1] = pick_rows(table, 0, k)
        slot_sends(k).start()
    r.xs[0, :slots, :] = pick_rows(table, 0, 0)

    def slot_forward(k):
        return remote(
            r.xs.at[k, pl.ds(0, slots)], r.xs.at[k, pl.ds(slots, slots)],
            r.sf_s.at[k - 1], r.sf_r.at[k - 1], partner,
        )

    def silu(values):
        return values / (1.0 + jnp.exp(-values))

    for name in ("sg", "su", "sd"):
        loads[name].wait()
    for q in range(2):
        if q == 1:
            rows_copy.wait_recv()
            r.xs[0, slots:, :] = pick_rows(slot_table(1), 1, 0)
        inputs = r.nrm[q]
        hidden = silu(jnp.dot(inputs, r.sg[...], preferred_element_type=f32))
        hidden = (hidden * jnp.dot(inputs, r.su[...], preferred_element_type=f32)).astype(bf16)
        r.shared[q] = jnp.dot(hidden, r.sd[...], preferred_element_type=f32).astype(bf16)
    shared_copy = remote(r.shared.at[1], r.shared.at[2], r.sh_s, r.sh_r, partner)
    shared_copy.start()

    spread_row = lax.broadcasted_iota(jnp.int32, (r.wq_t.shape[0], heads * LANES), 0)
    spread_col = lax.broadcasted_iota(jnp.int32, (r.wq_t.shape[0], heads * LANES), 1)
    in_head = spread_col % LANES
    spread = (
        (in_head < NOPE + ROPE_DIM)
        & (spread_row == (spread_col // LANES) * (NOPE + ROPE_DIM) + in_head)
    ).astype(f32).astype(bf16)
    r.wq[...] = lax.dot_general(
        r.wq_t[...], spread, (((0,), (0,)), ((), ())), preferred_element_type=f32
    ).astype(bf16)
    loads["q"].wait()

    def project(i, _):
        here = pl.ds(pl.multiple_of(i * tile, tile), tile)
        values = r.q_raw[here, :].astype(f32)
        scale = lax.rsqrt(jnp.mean(values * values, -1, keepdims=True) + norm_eps)
        normed = (values * scale * r.q_gain[...]).astype(bf16)
        projected = jnp.dot(normed, r.wq[...], preferred_element_type=f32)
        for head in range(heads):
            straight = projected[:, head * LANES : (head + 1) * LANES]
            r.q_all[head, here, :] = rotated(
                straight, r.cosine[here, :], r.sine[here, :]
            ).astype(bf16)
        return 0

    lax.fori_loop(0, 4, project, 0)

    lane_half = lax.broadcasted_iota(jnp.int32, (half, LANES), 1)

    def expand(k):
        for h in range(2):
            source = r.ropes[k, h].astype(f32)
            pieces = [
                pltpu.roll(source, (NOPE - ROPE_DIM * g) % LANES, 1) for g in range(4)
            ]
            turned = jnp.concatenate(pieces, 0)
            turned = jnp.where(
                (lane_half >= NOPE) & (lane_half < NOPE + ROPE_DIM), turned, 0.0
            )
            product = jnp.dot(
                r.kvs[k, h * half : (h + 1) * half, :], r.wkv[...], preferred_element_type=f32
            )
            start = pl.ds(pl.multiple_of(k * rows + h * half, half), half)
            for head in range(heads):
                pair = product[:, head * LANES : (head + 1) * LANES]
                r.k_all[head, start, :] = jnp.where(lane_half < NOPE, pair, turned).astype(bf16)
                r.v_all[head, start, :] = jnp.where(lane_half == 0, 1.0, pair).astype(bf16)

    def attend(queries, carry, start, size, masked):
        scored = [
            lax.dot_general(
                queries[head],
                r.k_all[head, pl.ds(start, size), :],
                (((1,), (1,)), ((), ())),
                preferred_element_type=f32,
            )
            for head in range(heads)
        ]
        result = []
        for head in range(heads):
            scores = scored[head]
            old_max, acc = carry[head]
            if masked is not None:
                row = lax.broadcasted_iota(jnp.int32, scores.shape, 0) + masked
                column = lax.broadcasted_iota(jnp.int32, scores.shape, 1)
                scores = jnp.where(column <= row, scores, -jnp.inf)
            new_max = jnp.maximum(old_max, jnp.max(scores, -1, keepdims=True))
            weights = jnp.exp2((scores - new_max) * factor).astype(bf16)
            product = jnp.dot(
                weights, r.v_all[head, pl.ds(start, size), :], preferred_element_type=f32
            )
            result.append((new_max, acc * jnp.exp2((old_max - new_max) * factor) + product))
        return tuple(result)

    expand(0)

    for i in range(4):
        here = slice(i * tile, (i + 1) * tile)
        queries = [r.q_all[head, here, :] for head in range(heads)]
        carry = tuple(
            (jnp.full((tile, 1), floor_value, f32), jnp.zeros((tile, LANES), f32))
            for head in range(heads)
        )
        carry = attend(queries, carry, 0, (i + 1) * tile, i * tile)
        for head in range(heads):
            r.top[head, here, :] = jnp.broadcast_to(carry[head][0], (tile, LANES))
            r.acc[head, here, :] = carry[head][1]

    for k in (1, 2, 3):

        @pl.when(ep_of(k) < e)
        def _(k=k):
            for copy, forward in zip(pack_copies(k), pack_forwards(k)):
                copy.wait_recv()
                forward.start()

    for k in (1, 2, 3):

        @pl.when(ep_of(k) < e)
        def _(k=k):
            for forward in pack_forwards(k):
                forward.wait_recv()
            expand(k)

    head_cols = heads * VDIM
    own_cols = pl.ds(pl.multiple_of(t * head_cols, head_cols), head_cols)

    def remote_tile(i, _):
        here = pl.ds(pl.multiple_of(i * tile, tile), tile)
        queries = [r.q_all[head, here, :] for head in range(heads)]
        carry = tuple(
            (r.top[head, here, :][:, :1], r.acc[head, here, :]) for head in range(heads)
        )
        carry = lax.fori_loop(
            0, e,
            lambda s, cc: attend(
                queries, cc, pl.multiple_of(rel_of(s) * rows, rows), rows, None
            ),
            carry,
        )
        outs = [acc[:, NOPE : NOPE + VDIM] / acc[:, :1] for _, acc in carry]
        r.mixers[here, own_cols] = jnp.concatenate(outs, -1).astype(bf16)
        for j in (3, 1, 2, 0):
            head_copy(i, j).start()
        return 0

    def depth_of(j):
        return (d + j) % depths

    def head_copy(i, j):
        device = partner if j == 0 else (e, depth_of(j) * 2 + c)
        here = pl.ds(pl.multiple_of(i * tile, tile), tile)
        return remote(
            r.mixers.at[here, own_cols], r.mixers.at[here, own_cols],
            r.h_s.at[i, j], r.h_r.at[i, j], device,
        )

    lax.fori_loop(0, 4, remote_tile, 0)

    def head_forward(j):
        source = ((d + depths - j) % depths) * 2 + c
        cols = pl.ds(pl.multiple_of(source * head_cols, head_cols), head_cols)
        return remote(
            r.mixers.at[:, cols], r.mixers.at[:, cols],
            r.hf_s.at[j - 1], r.hf_r.at[j - 1], partner,
        )

    for k in (3, 2, 1):
        slot_sends(k).wait_recv()
        slot_forward(k).start()
    for name in ("eg", "eu", "ed"):
        loads[name].wait()

    quarter = width // 4
    chunks = [(0, 2 * quarter), (2 * quarter, quarter), (3 * quarter, quarter)]

    def partial_copy(n, k):
        cols = pl.ds(*chunks[n])
        return remote(
            r.theirs.at[k, :, cols], r.pair.at[k, :, cols],
            r.ex_s.at[n, k], r.ex_r.at[n, k], partner,
        )

    def return_copy(n, k):
        cols = pl.ds(*chunks[n])
        return remote(
            r.sums.at[k, pl.ds(0, slots), cols], r.back.at[k, pl.ds(0, slots), cols],
            r.rt_s.at[n, k - 1], r.rt_r.at[n, k - 1], (ep_of(k), t),
        )

    hidden_units = r.eg.shape[1]
    step = min(256, hidden_units)

    def expert_hidden(k):
        inputs = r.xs[k]
        for n in range(0, hidden_units, step):
            gate = silu(jnp.dot(inputs, r.eg[:, n : n + step], preferred_element_type=f32))
            up = jnp.dot(inputs, r.eu[:, n : n + step], preferred_element_type=f32)
            r.hid[k, :, n : n + step] = (gate * up).astype(bf16)

    def expert_down(n, k):
        for start in range(chunks[n][0], sum(chunks[n]), quarter):
            cols = slice(start, start + quarter)
            product = jnp.dot(
                r.hid[k], r.ed[:, cols], preferred_element_type=f32
            ).astype(bf16)
            r.ours[k, :, cols] = product[:slots]
            r.theirs[k, :, cols] = product[slots:]
        partial_copy(n, k).start()

    def finish(n, k):
        cols = slice(chunks[n][0], sum(chunks[n]))
        partial_copy(n, k).wait_recv()
        r.sums[k, :slots, cols] = (
            r.ours[k, :, cols].astype(f32) + r.pair[k, :, cols].astype(f32)
        ).astype(bf16)

    def first_pass(i, _):
        k = 3 - i

        @pl.when(k > 0)
        def _():
            slot_forward(k).wait_recv()

        expert_hidden(k)
        expert_down(0, k)

        @pl.when(i > 0)
        def _():
            finish(0, k + 1)
            return_copy(0, k + 1).start()

        return 0

    r.back[:, slots:, :] = jnp.zeros((4, r.back.shape[1] - slots, width), bf16)
    r.sums[0, slots:, :] = jnp.zeros((r.back.shape[1] - slots, width), bf16)
    lax.fori_loop(0, 4, first_pass, 0)
    for n in (1, 2):

        def later_pass(i, _, n=n):
            k = 3 - i
            expert_down(n, k)

            @pl.when(i == 0)
            def _():
                finish(n - 1, 0)

            @pl.when(i > 0)
            def _():
                finish(n, k + 1)
                return_copy(n, k + 1).start()

            return 0

        lax.fori_loop(0, 4, later_pass, 0)
    finish(2, 0)
    shared_copy.wait_recv()

    tags = gather_rows(0)
    routes, weight = tags[:, :top], tags[:, top : 2 * top]
    factors = [
        jnp.sum(
            jnp.where(routes == ep_of(k).astype(f32), weight, 0.0), -1, keepdims=True
        )
        for k in range(4)
    ]

    def z_copy(n, j):
        there = depth_of(j)
        cols = pl.ds(*chunks[n])
        return remote(
            r.zs.at[pl.ds(pl.multiple_of(there * MOE_DEV, MOE_DEV), MOE_DEV), cols],
            r.zr.at[j - 1, :, cols],
            r.z_s.at[n, j - 1], r.z_r.at[n, j - 1], (e, there * 2 + c),
        )

    def combine(n):
        for k in (3, 2, 1):
            return_copy(n, k).wait_recv()
        for start in range(chunks[n][0], sum(chunks[n]), quarter):
            cols = slice(start, start + quarter)
            total = r.shared[0, :, cols].astype(f32) + r.shared[2, :, cols].astype(f32)
            for k in range(4):
                source = r.back if k > 0 else r.sums
                total = total + factors[k] * jnp.dot(
                    r.onehot[k], source[k, :, cols], preferred_element_type=f32
                )
            r.zs[:, cols] = total.astype(bf16)
        for j in range(1, depths):
            z_copy(n, j).start()

    def mix(i, _):
        here = pl.ds(pl.multiple_of(i * tile, tile), tile)
        r.mixed[here, :] = jnp.dot(
            r.mixers[here, :], r.wo[...], preferred_element_type=f32
        ).astype(bf16)
        return 0

    combine(0)
    combine(1)
    for j in range(1, depths):
        for i in range(4):
            head_copy(i, j).wait_recv()
        head_forward(j).start()
    combine(2)
    loads["wo"].wait()
    for i in range(4):
        head_copy(i, 0).wait_recv()
    for j in range(1, depths):
        head_forward(j).wait_recv()
    lax.fori_loop(0, 4, mix, 0)
    for n in range(len(chunks)):
        for j in range(1, depths):
            z_copy(n, j).wait_recv()
    final = r.zs[pl.ds(pl.multiple_of(d * MOE_DEV, MOE_DEV), MOE_DEV), :].astype(f32)
    for j in range(1, depths):
        final = final + r.zr[j - 1].astype(f32)
    r.moe_out[...] = final.astype(bf16)

    for k in (1, 2, 3):

        @pl.when(ep_of(k) > e)
        def _(k=k):
            for copy in pack_copies(k):
                copy.wait_send()

        @pl.when(ep_of(k) < e)
        def _(k=k):
            for copy in pack_forwards(k):
                copy.wait_send()

        slot_sends(k).wait_send()
        slot_forward(k).wait_send()
        for n in range(len(chunks)):
            return_copy(n, k).wait_send()
    shared_copy.wait_send()
    rows_copy.wait_send()
    for k in range(4):
        for n in range(len(chunks)):
            partial_copy(n, k).wait_send()
    for j in range(depths):
        for i in range(4):
            head_copy(i, j).wait_send()
    for j in range(1, depths):
        head_forward(j).wait_send()
        for n in range(len(chunks)):
            z_copy(n, j).wait_send()


def rotary_constant(total, per_device):
    halfway = ROPE_DIM // 2
    inverse = (
        np.float32(rotary_base)
        ** (-(np.arange(halfway, dtype=np.float32) * np.float32(2.0) / np.float32(ROPE_DIM)))
    ).astype(np.float32)
    angles = (np.arange(total, dtype=np.float32)[:, None] * inverse[None, :]).astype(np.float32)
    angles = angles.astype(np.float64)
    both = np.concatenate([np.cos(angles), np.sin(angles)], 1).astype(np.float32)
    groups = both.reshape(-1, LANES // ROPE_DIM, per_device * ROPE_DIM // LANES, ROPE_DIM)
    return groups.transpose(0, 2, 1, 3).reshape(-1, LANES)


def fused_body(
    q_latent,
    kv_latent,
    rope_key,
    q_gain,
    kv_gain,
    w_query,
    w_keyval,
    w_output,
    moe_input,
    moe_gain,
    routes,
    route_weight,
    expert_gate,
    expert_up,
    expert_down,
    shared_gate,
    shared_up,
    shared_down,
):
    rows, qlat = q_latent.shape
    latent = kv_latent.shape[1]
    ep_count = lax.axis_size("ep")
    tp_count = lax.axis_size("tp")
    heads = w_query.shape[1] // (NOPE + ROPE_DIM)
    tokens, width = moe_input.shape
    side = tokens // 2
    depths = tp_count // 2
    hidden = expert_gate.shape[2]
    shared_hidden = shared_gate.shape[1]
    top = routes.shape[1]
    capacity = 3 * MOE_DEV * top // (2 * ep_count)
    slots = depths * capacity
    columns = w_output.shape[1]
    bf16, f32 = jnp.bfloat16, jnp.float32
    table = jnp.asarray(rotary_constant(rows * ep_count, rows))
    hbm = pl.BlockSpec(memory_space=pltpu.HBM)
    vmem = pl.BlockSpec(memory_space=pltpu.VMEM)
    inputs = [
        ("q_hbm", q_latent, hbm),
        ("kv_hbm", kv_latent, hbm),
        ("table_hbm", table, hbm),
        ("moe_hbm", moe_input, hbm),
        ("eg_hbm", expert_gate, hbm),
        ("eu_hbm", expert_up, hbm),
        ("ed_hbm", expert_down, hbm),
        ("sg_hbm", shared_gate, hbm),
        ("su_hbm", shared_up, hbm),
        ("sd_hbm", shared_down, hbm),
        ("wo_hbm", w_output, hbm),
        ("rope_t", rope_key.T, vmem),
        ("q_gain", q_gain.reshape(1, -1), vmem),
        ("kv_gain", kv_gain.reshape(1, -1), vmem),
        ("wq_t", w_query.T, vmem),
        ("wkv", w_keyval, vmem),
        ("moe_gain", moe_gain.reshape(1, -1), vmem),
        ("routes_t", routes.T, vmem),
        ("weight_t", route_weight.T, vmem),
    ]
    outputs = [("mixed", (rows, columns)), ("moe_out", (MOE_DEV, width))]
    dma = pltpu.SemaphoreType.DMA
    scratch = [
        ("kv_raw", pltpu.VMEM((rows, latent), bf16)),
        ("q_raw", pltpu.VMEM((rows, qlat), bf16)),
        ("table", pltpu.VMEM((rows // 4, LANES), f32)),
        ("tags", pltpu.VMEM((LANES, tokens), f32)),
        ("tagged", pltpu.VMEM((tokens, LANES), f32)),
        ("wq", pltpu.VMEM((qlat, heads * LANES), bf16)),
        ("cosine", pltpu.VMEM((rows, LANES), f32)),
        ("sine", pltpu.VMEM((rows, LANES), f32)),
        ("kvs", pltpu.VMEM((4, rows, latent), bf16)),
        ("ropes", pltpu.VMEM((4, 2, rows // 8, LANES), bf16)),
        ("nrm", pltpu.VMEM((2, side, width), bf16)),
        ("onehot", pltpu.VMEM((4, side, LANES), bf16)),
        ("snd", pltpu.VMEM((3, slots, width), bf16)),
        ("xs", pltpu.VMEM((4, 2 * slots, width), bf16)),
        ("shared", pltpu.VMEM((3, side, width), bf16)),
        ("q_all", pltpu.VMEM((heads, rows, LANES), bf16)),
        ("k_all", pltpu.VMEM((heads, 4 * rows, LANES), bf16)),
        ("v_all", pltpu.VMEM((heads, 4 * rows, LANES), bf16)),
        ("top", pltpu.VMEM((heads, rows, LANES), f32)),
        ("acc", pltpu.VMEM((heads, rows, LANES), f32)),
        ("mixers", pltpu.VMEM((rows, tp_count * heads * VDIM), bf16)),
        ("ours", pltpu.VMEM((4, slots, width), bf16)),
        ("theirs", pltpu.VMEM((4, slots, width), bf16)),
        ("pair", pltpu.VMEM((4, slots, width), bf16)),
        ("sums", pltpu.VMEM((4, LANES, width), bf16)),
        ("hid", pltpu.VMEM((4, 2 * slots, hidden), bf16)),
        ("back", pltpu.VMEM((4, LANES, width), bf16)),
        ("zs", pltpu.VMEM((side, width), bf16)),
        ("zr", pltpu.VMEM((depths - 1, MOE_DEV, width), bf16)),
        ("eg", pltpu.VMEM((width, hidden), bf16)),
        ("eu", pltpu.VMEM((width, hidden), bf16)),
        ("ed", pltpu.VMEM((hidden, width), bf16)),
        ("sg", pltpu.VMEM((width, shared_hidden), bf16)),
        ("su", pltpu.VMEM((width, shared_hidden), bf16)),
        ("sd", pltpu.VMEM((shared_hidden, width), bf16)),
        ("wo", pltpu.VMEM(w_output.shape, bf16)),
        ("ld", dma((10 + depths,))),
        ("pk_s", dma((3, 2))),
        ("pk_r", dma((3, 2))),
        ("pf_s", dma((3, 2))),
        ("pf_r", dma((3, 2))),
        ("sl_s", dma((3,))),
        ("sl_r", dma((3,))),
        ("sf_s", dma((3,))),
        ("sf_r", dma((3,))),
        ("rc_s", dma),
        ("rc_r", dma),
        ("sh_s", dma),
        ("sh_r", dma),
        ("ex_s", dma((3, 4))),
        ("ex_r", dma((3, 4))),
        ("rt_s", dma((3, 3))),
        ("rt_r", dma((3, 3))),
        ("h_s", dma((4, depths))),
        ("h_r", dma((4, depths))),
        ("hf_s", dma((depths - 1,))),
        ("hf_r", dma((depths - 1,))),
        ("z_s", dma((3, depths - 1))),
        ("z_r", dma((3, depths - 1))),
    ]
    names = [x[0] for x in inputs] + [x[0] for x in outputs] + [x[0] for x in scratch]
    mixed, moe_out = pl.pallas_call(
        lambda *refs: fused_kernel(names, *refs),
        out_shape=[jax.ShapeDtypeStruct(shape, bf16) for _, shape in outputs],
        in_specs=[spec for _, _, spec in inputs],
        out_specs=[vmem] * len(outputs),
        scratch_shapes=[spec for _, spec in scratch],
        compiler_params=pltpu.CompilerParams(
            collective_id=0,
            has_side_effects=True,
            vmem_limit_bytes=60 * 1024 * 1024,
        ),
        name="fused",
    )(*[value for _, value, _ in inputs])
    return (mixed, moe_out)


def solution(mesh):
    in_specs = (
        P("ep", None),
        P("ep", None),
        P("ep", None),
        P(),
        P(),
        P(None, "tp"),
        P(None, "tp"),
        P(None, "tp"),
        P("ep", None),
        P(),
        P("ep", None),
        P("ep", None),
        P("ep", None, "tp"),
        P("ep", None, "tp"),
        P("ep", "tp", None),
        P(None, "tp"),
        P(None, "tp"),
        P("tp", None),
    )
    out_specs = (P("ep", "tp"), P(("ep", "tp"), None))
    chosen = fused_body if mesh.shape["ep"] == 4 else body
    return jax.shard_map(
        chosen, mesh=mesh, in_specs=in_specs, out_specs=out_specs, check_vma=False
    )
```

```python
import jax
import jax.numpy as jnp
import numpy as np
from jax import lax
from jax.experimental import pallas as pl
from jax.experimental.pallas import tpu as pltpu
from jax.sharding import PartitionSpec as P

NOPE = 64
ROPE_DIM = 32
VDIM = 64
MOE_DEV = 32


norm_eps = 1e-06
layer_eps = 1e-05
rotary_base = 10000.0
floor_value = -1e30


def rms_scale(values, gain):
    widened = values.astype(jnp.float32)
    return (
        widened * lax.rsqrt(jnp.mean(widened * widened, -1, keepdims=True) + norm_eps) * gain
    ).astype(jnp.bfloat16)


def layer_scale(values, gain):
    widened = values.astype(jnp.float32)
    centred = widened - jnp.mean(widened, -1, keepdims=True)
    return (
        centred * lax.rsqrt(jnp.mean(centred * centred, -1, keepdims=True) + layer_eps) * gain
    ).astype(jnp.bfloat16)


def rotary_tables(positions):
    halfway = ROPE_DIM // 2
    inverse = rotary_base ** (-(jnp.arange(halfway, dtype=jnp.float32) * 2.0 / ROPE_DIM))
    angles = positions.astype(jnp.float32)[:, None] * inverse[None, :]
    return (jnp.cos(angles), jnp.sin(angles))


def rotate(values, cosine_table, sine_table):
    halfway = values.shape[-1] // 2
    first_half = values[..., :halfway]
    second_half = values[..., halfway:]
    return jnp.concatenate(
        [
            first_half * cosine_table - second_half * sine_table,
            second_half * cosine_table + first_half * sine_table,
        ],
        -1,
    )


def block_stats(query_block, query_pos, keyvals, rotated_keys, key_pos):
    scale = float(NOPE + ROPE_DIM) ** (-0.5)
    scores = jnp.einsum(
        "qhd,khd->hqk",
        query_block[..., :NOPE],
        keyvals[..., :NOPE],
        preferred_element_type=jnp.float32,
    )
    scores = (
        scores
        + jnp.einsum(
            "qhd,kd->hqk", query_block[..., NOPE:], rotated_keys, preferred_element_type=jnp.float32
        )
    ) * scale
    allowed = key_pos[None, :] <= query_pos[:, None]
    scores = jnp.where(allowed[None], scores, -jnp.inf)
    block_max = jnp.max(scores, -1)
    weights = jnp.exp(scores - block_max[..., None])
    block_sum = jnp.sum(weights, -1)
    attended = jnp.einsum(
        "hqk,khd->qhd",
        weights.astype(jnp.bfloat16),
        keyvals[..., NOPE:],
        preferred_element_type=jnp.float32,
    ).astype(jnp.bfloat16)
    return (block_max.T, block_sum.T, attended)


def merge_block(carried, stats):
    running_max, running_sum, running_acc = carried
    block_max, block_sum, attended = stats
    new_max = jnp.maximum(running_max, block_max)
    old_weight = jnp.exp(running_max - new_max)
    new_weight = jnp.exp(block_max - new_max)
    return (
        new_max,
        running_sum * old_weight + block_sum * new_weight,
        running_acc * old_weight[..., None] + attended.astype(jnp.float32) * new_weight[..., None],
    )


def body(
    q_latent,
    kv_latent,
    rope_key,
    q_gain,
    kv_gain,
    w_query,
    w_keyval,
    w_output,
    moe_input,
    moe_gain,
    routes,
    route_weight,
    expert_gate,
    expert_up,
    expert_down,
    shared_gate,
    shared_up,
    shared_down,
):
    row_count = q_latent.shape[0]
    own_index = lax.axis_index("ep")
    ep_count = lax.axis_size("ep")
    tp_count = lax.axis_size("tp")
    positions = own_index * row_count + jnp.arange(row_count, dtype=jnp.int32)
    cosine_table, sine_table = rotary_tables(positions)
    q_normed = rms_scale(q_latent, q_gain)
    kv_normed = rms_scale(kv_latent, kv_gain)
    key_rotated = rotate(rope_key.astype(jnp.float32), cosine_table, sine_table).astype(
        jnp.bfloat16
    )
    heads_local = w_query.shape[1] // (NOPE + ROPE_DIM)
    projected = jnp.dot(q_normed, w_query, preferred_element_type=jnp.float32)
    projected = projected.reshape(row_count, heads_local, NOPE + ROPE_DIM)
    queries = jnp.concatenate(
        [
            projected[..., :NOPE],
            rotate(projected[..., NOPE:], cosine_table[:, None, :], sine_table[:, None, :]),
        ],
        -1,
    ).astype(jnp.bfloat16)

    def expand_keys(latent_rows):
        expanded = jnp.dot(latent_rows, w_keyval, preferred_element_type=jnp.float32).astype(
            jnp.bfloat16
        )
        return expanded.reshape(latent_rows.shape[0], heads_local, NOPE + VDIM)

    initial = (
        jnp.full((row_count, heads_local), floor_value, jnp.float32),
        jnp.zeros((row_count, heads_local), jnp.float32),
        jnp.zeros((row_count, heads_local, VDIM), jnp.float32),
    )
    carried = initial
    latent_piece = lax.all_gather(kv_normed, "ep", axis=0, tiled=True)
    rotated_piece = lax.all_gather(key_rotated, "ep", axis=0, tiled=True)
    block_count = latent_piece.shape[0] // row_count

    def visit_block(inner, offset):

        def live(current):
            latent_rows = lax.dynamic_slice_in_dim(latent_piece, offset * row_count, row_count, 0)
            rotated_rows = lax.dynamic_slice_in_dim(rotated_piece, offset * row_count, row_count, 0)
            key_pos = offset * row_count + jnp.arange(row_count, dtype=jnp.int32)
            stats = block_stats(queries, positions, expand_keys(latent_rows), rotated_rows, key_pos)
            return merge_block(current, stats)

        def skipped(current):
            return current

        return (lax.cond(offset <= own_index, live, skipped, inner), None)

    carried, unused = lax.scan(visit_block, carried, jnp.arange(block_count, dtype=jnp.int32))
    running_max, running_sum, running_acc = carried
    heads_out = (
        (running_acc / running_sum[..., None])
        .astype(jnp.bfloat16)
        .reshape(row_count, heads_local * VDIM)
    )
    mixed = jnp.dot(
        lax.all_gather(heads_out, "tp", axis=1, tiled=True),
        w_output,
        preferred_element_type=jnp.float32,
    )
    mixed = mixed.astype(jnp.bfloat16)
    width = moe_input.shape[1]
    top_count = routes.shape[1]
    local_experts = expert_gate.shape[0]
    expert_count = local_experts * ep_count
    capacity = max(2, 3 * MOE_DEV * top_count // (2 * expert_count))
    normed = layer_scale(moe_input, moe_gain)
    entries = routes.reshape(tp_count, MOE_DEV * top_count)
    onehot = (entries[..., None] == jnp.arange(expert_count, dtype=jnp.int32)).astype(jnp.int32)
    earlier = jnp.cumsum(onehot, 1) - onehot
    rank_in = jnp.sum(earlier * onehot, -1)
    block_ids = jnp.arange(tp_count, dtype=jnp.int32)[:, None]
    slot_of = ((entries * tp_count + block_ids) * capacity + rank_in).reshape(-1, top_count)
    token_ids = jnp.arange(tp_count * MOE_DEV * top_count, dtype=jnp.int32) // top_count
    slot_token = (
        jnp.full((expert_count * tp_count * capacity,), -1, jnp.int32)
        .at[slot_of.reshape(-1)]
        .set(token_ids)
    )
    outgoing = jnp.where(
        (slot_token >= 0)[:, None], normed[jnp.maximum(slot_token, 0)], jnp.zeros((), jnp.bfloat16)
    )
    outgoing = outgoing.reshape(ep_count, local_experts, tp_count, capacity, width)
    arrived = lax.all_to_all(outgoing, "ep", split_axis=0, concat_axis=0, tiled=True)
    slot_rows = arrived.shape[3]
    inputs = arrived[:, 0].reshape(-1, width)
    hidden = jax.nn.silu(jnp.dot(inputs, expert_gate[0], preferred_element_type=jnp.float32))
    hidden = (hidden * jnp.dot(inputs, expert_up[0], preferred_element_type=jnp.float32)).astype(
        jnp.bfloat16
    )
    output = jnp.dot(hidden, expert_down[0], preferred_element_type=jnp.float32)
    results = [output.astype(jnp.bfloat16).reshape(ep_count, tp_count, slot_rows, width)]
    partial_value = jnp.stack(results, 1)
    shared_hidden = jax.nn.silu(jnp.dot(normed, shared_gate, preferred_element_type=jnp.float32))
    shared_hidden = (
        shared_hidden * jnp.dot(normed, shared_up, preferred_element_type=jnp.float32)
    ).astype(jnp.bfloat16)
    shared_part = jnp.dot(shared_hidden, shared_down, preferred_element_type=jnp.float32).astype(
        jnp.bfloat16
    )
    slot_total, shared_total = (
        lax.psum_scatter(
            partial_value.astype(jnp.float32).astype(jnp.bfloat16),
            "tp",
            scatter_dimension=2,
            tiled=True,
        ).astype(jnp.float32),
        lax.psum_scatter(
            shared_part.astype(jnp.float32)
            .reshape(1, 1, tp_count, MOE_DEV, width)
            .astype(jnp.bfloat16),
            "tp",
            scatter_dimension=2,
            tiled=True,
        ).astype(jnp.float32),
    )
    arrived_sums = lax.all_to_all(
        slot_total.astype(jnp.bfloat16), "ep", split_axis=0, concat_axis=0, tiled=True
    ).astype(slot_total.dtype)
    own_block = lax.axis_index("tp")
    own_entries = lax.dynamic_slice_in_dim(routes, own_block * MOE_DEV, MOE_DEV, 0)
    own_rank = lax.dynamic_slice_in_dim(
        rank_in.reshape(-1, top_count), own_block * MOE_DEV, MOE_DEV, 0
    )
    own_weight = lax.dynamic_slice_in_dim(route_weight, own_block * MOE_DEV, MOE_DEV, 0)
    picked = arrived_sums.reshape(-1, width)[own_entries * capacity + own_rank]
    moe_out = (
        jnp.sum(own_weight[..., None] * picked, 1) + shared_total.reshape(MOE_DEV, width)
    ).astype(jnp.bfloat16)
    return (mixed, moe_out)


LANES = 128
LOG2E = 1.4426950408889634
MESH = pl.DeviceIdType.MESH


class Refs:
    pass


def fused_kernel(names, *refs):
    r = Refs()
    for name, ref in zip(names, refs):
        setattr(r, name, ref)
    f32, bf16 = jnp.float32, jnp.bfloat16
    e = lax.axis_index("ep")
    t = lax.axis_index("tp")
    c = t % 2
    d = t // 2
    ex, ey = e % 2, e // 2
    partner = (e, t + 1 - 2 * c)
    rows = r.kv_hbm.shape[0]
    half = rows // 2
    tile = rows // 4
    eighth = rows // 8
    latent = r.kv_hbm.shape[1]
    heads = r.k_all.shape[0]
    width = r.moe_hbm.shape[1]
    slots = r.xs.shape[1] // 2
    side = r.nrm.shape[1]
    depths = side // MOE_DEV
    capacity = slots // depths
    factor = float(NOPE + ROPE_DIM) ** (-0.5) * LOG2E
    halfway = ROPE_DIM // 2

    def ep_of(k):
        return ((ey + k // 2) % 2) * 2 + (ex + k % 2) % 2

    def rel_of(source):
        return ((source // 2 + ey) % 2) * 2 + (source % 2 + ex) % 2

    def remote(src, dst, send, recv, device):
        return pltpu.make_async_remote_copy(
            src_ref=src, dst_ref=dst, send_sem=send, recv_sem=recv,
            device_id=device, device_id_type=MESH,
        )

    loads = {}

    def load(name, src, dst, sem):
        copy = pltpu.make_async_copy(src, dst, r.ld.at[sem])
        copy.start()
        loads[name] = copy

    load("kv", r.kv_hbm, r.kv_raw, 0)
    load("table", r.table_hbm.at[pl.ds(pl.multiple_of(e * tile, tile), tile)], r.table, 1)
    for j in range(depths):
        load(
            f"moe{j}",
            r.moe_hbm.at[pl.ds(pl.multiple_of((2 * j + c) * MOE_DEV, MOE_DEV), MOE_DEV)],
            r.nrm.at[0, pl.ds(j * MOE_DEV, MOE_DEV)],
            2 + j,
        )
    first = 2 + depths
    load("q", r.q_hbm, r.q_raw, first)
    load("sg", r.sg_hbm, r.sg, first + 1)
    load("su", r.su_hbm, r.su, first + 2)
    load("sd", r.sd_hbm, r.sd, first + 3)
    load("eg", r.eg_hbm.at[0], r.eg, first + 4)
    load("eu", r.eu_hbm.at[0], r.eu, first + 5)
    load("ed", r.ed_hbm.at[0], r.ed, first + 6)
    load("wo", r.wo_hbm, r.wo, first + 7)

    barrier = pltpu.get_barrier_semaphore()
    peers = [partner] + [(ep_of(k), t) for k in (1, 2, 3)]
    peers += [(e, ((d + j) % depths) * 2 + c) for j in range(1, depths)]
    for peer in peers:
        pl.semaphore_signal(barrier, inc=1, device_id=peer, device_id_type=MESH)

    lane = lax.broadcasted_iota(jnp.int32, (tile, LANES), 1)
    low = (lane >= NOPE) & (lane < NOPE + halfway)
    high = (lane >= NOPE + halfway) & (lane < NOPE + ROPE_DIM)

    def rotated(values, cosine, sine):
        swapped = jnp.where(
            lane < NOPE + halfway,
            pltpu.roll(values, LANES - halfway, 1),
            pltpu.roll(values, halfway, 1),
        )
        return values * cosine + swapped * sine

    loads["table"].wait()
    for i in range(4):
        turned = pltpu.roll(r.table[...], (NOPE - ROPE_DIM * i) % LANES, 1)
        later = pltpu.roll(turned, halfway, 1)
        sooner = pltpu.roll(turned, LANES - halfway, 1)
        here = pl.ds(i * tile, tile)
        r.cosine[here, :] = jnp.where(
            lane < NOPE, 1.0, jnp.where(low, turned, jnp.where(high, later, 0.0))
        )
        r.sine[here, :] = jnp.where(low, -sooner, jnp.where(high, turned, 0.0))

    r.tags[...] = jnp.zeros(r.tags.shape, f32)
    top = r.routes_t.shape[0]
    r.tags[:top, :] = r.routes_t[...].astype(f32)
    r.tags[top : 2 * top, :] = r.weight_t[...]
    r.tagged[...] = r.tags[...].T

    place = (
        lax.broadcasted_iota(jnp.int32, (ROPE_DIM, LANES), 0) + NOPE
        == lax.broadcasted_iota(jnp.int32, (ROPE_DIM, LANES), 1)
    ).astype(f32).astype(bf16)

    loads["kv"].wait()
    packed = [jnp.zeros((eighth, LANES), f32) for _ in range(2)]
    for i in range(4):
        here = pl.ds(i * tile, tile)
        values = r.kv_raw[here, :].astype(f32)
        scale = lax.rsqrt(jnp.mean(values * values, -1, keepdims=True) + norm_eps)
        r.kvs[0, here, :] = (values * scale * r.kv_gain[...]).astype(bf16)
        straight = lax.dot_general(
            r.rope_t[:, i * tile : (i + 1) * tile], place,
            (((0,), (0,)), ((), ())), preferred_element_type=f32,
        )
        turned = rotated(straight, r.cosine[here, :], r.sine[here, :])
        for part in range(2):
            g = 2 * (i % 2) + part
            piece = turned[part * eighth : (part + 1) * eighth]
            packed[i // 2] += pltpu.roll(piece, (ROPE_DIM * g - NOPE) % LANES, 1)
    for h in range(2):
        r.ropes[0, h] = packed[h].astype(bf16)

    pl.semaphore_wait(barrier, len(peers))

    own_half = pl.ds(pl.multiple_of(c * half, half), half)

    kv_part, rope_part = half // depths, eighth // depths

    def depth_of(j):
        return (d + j) % depths

    def z_peer(j):
        return (e, depth_of(j) * 2 + c)

    kv_quarter = pl.ds(pl.multiple_of(c * half + d * kv_part, kv_part), kv_part)
    rope_quarter = pl.ds(pl.multiple_of(d * rope_part, rope_part), rope_part)

    def pack_copies(k):
        device = (ep_of(k), t)
        kv_rows, rope_rows = (kv_quarter, rope_quarter) if k == 3 else (own_half, slice(None))
        return [
            remote(r.kvs.at[0, kv_rows], r.kvs.at[k, kv_rows],
                   r.pk_s.at[k - 1, 0], r.pk_r.at[k - 1, 0], device),
            remote(r.ropes.at[0, c, rope_rows], r.ropes.at[k, c, rope_rows],
                   r.pk_s.at[k - 1, 1], r.pk_r.at[k - 1, 1], device),
        ]

    def pack_spreads(j):
        return [
            remote(r.kvs.at[3, kv_quarter], r.kvs.at[3, kv_quarter],
                   r.ps_s.at[j - 1, 0], r.ps_r.at[j - 1, 0], z_peer(j)),
            remote(r.ropes.at[3, c, rope_quarter], r.ropes.at[3, c, rope_quarter],
                   r.ps_s.at[j - 1, 1], r.ps_r.at[j - 1, 1], z_peer(j)),
        ]

    def spread_packs():
        for copy in pack_copies(3):
            copy.wait_recv()
        for j in range(1, depths):
            for copy in pack_spreads(j):
                copy.start()

    def pack_forwards(k):
        return [
            remote(r.kvs.at[k, own_half], r.kvs.at[k, own_half],
                   r.pf_s.at[k - 1, 0], r.pf_r.at[k - 1, 0], partner),
            remote(r.ropes.at[k, c], r.ropes.at[k, c],
                   r.pf_s.at[k - 1, 1], r.pf_r.at[k - 1, 1], partner),
        ]

    for k in (3, 2, 1):

        @pl.when(ep_of(k) > e)
        def _(k=k):
            for copy in pack_copies(k):
                copy.start()

    for j in range(depths):
        loads[f"moe{j}"].wait()

    chunk = 16

    def norm_rows(i, _):
        here = pl.ds(pl.multiple_of(i * chunk, chunk), chunk)
        values = r.nrm[0, here, :].astype(f32)
        centred = values - jnp.mean(values, -1, keepdims=True)
        scale = lax.rsqrt(jnp.mean(centred * centred, -1, keepdims=True) + layer_eps)
        r.nrm[0, here, :] = (centred * scale * r.moe_gain[...]).astype(bf16)
        return 0

    lax.fori_loop(0, side // chunk, norm_rows, 0, unroll=2)
    rows_copy = remote(r.nrm.at[0], r.nrm.at[1], r.rc_s, r.rc_r, partner)
    rows_copy.start()

    row_id = lax.broadcasted_iota(jnp.int32, (side, side), 0)
    col_id = lax.broadcasted_iota(jnp.int32, (side, side), 1)
    earlier = (
        (col_id < row_id) & (col_id // MOE_DEV == row_id // MOE_DEV)
    ).astype(f32).astype(bf16)

    def gather_rows(q):
        return jnp.concatenate(
            [
                r.tagged[pl.ds(pl.multiple_of((2 * j + (c + q) % 2) * MOE_DEV, MOE_DEV), MOE_DEV), :]
                for j in range(depths)
            ],
            0,
        )

    lane_side = lax.broadcasted_iota(jnp.int32, (side, LANES), 1)
    block_of = lax.broadcasted_iota(jnp.int32, (side, LANES), 0) // MOE_DEV
    slot_cols = pl.ds(pl.multiple_of(d * (width // depths), width // depths), width // depths)

    def slot_sends(k):
        cols = slot_cols if k == 3 else slice(None)
        return remote(
            r.snd.at[k - 1, :, cols], r.xs.at[k, pl.ds(0, slots), cols],
            r.sl_s.at[k - 1], r.sl_r.at[k - 1], (ep_of(k), t),
        )

    def slot_spread(j):
        there = r.xs.at[3, pl.ds(0, slots), slot_cols]
        return remote(there, there, r.ss_s.at[j - 1], r.ss_r.at[j - 1], z_peer(j))

    def spread_slots():
        slot_sends(3).wait_recv()
        for j in range(1, depths):
            slot_spread(j).start()

    def slot_table(q):
        tags = gather_rows(q)
        named = lane_side < 0
        for k in range(top):
            named = named | (tags[:, k : k + 1] == lane_side.astype(f32))
        rank = jnp.dot(
            earlier, named.astype(f32).astype(bf16), preferred_element_type=f32
        )
        return jnp.where(named, rank + (block_of * capacity).astype(f32), -1.0)

    def pick_rows(slot, q, k):
        mine = jnp.sum(jnp.where(lane_side == ep_of(k), slot, 0.0), -1, keepdims=True)
        onehot = (mine == lane_side.astype(f32)).astype(f32)
        if q == 0:
            r.onehot[k] = onehot.astype(bf16)
        return jnp.dot(
            onehot.T.astype(bf16), r.nrm[q], preferred_element_type=f32
        )[:slots].astype(bf16)

    table = slot_table(0)
    for k in (3, 2, 1):
        r.snd[k - 1] = pick_rows(table, 0, k)
        slot_sends(k).start()
    r.xs[0, :slots, :] = pick_rows(table, 0, 0)

    def slot_forward(k):
        return remote(
            r.xs.at[k, pl.ds(0, slots)], r.xs.at[k, pl.ds(slots, slots)],
            r.sf_s.at[k - 1], r.sf_r.at[k - 1], partner,
        )

    def silu(values):
        return values / (1.0 + jnp.exp(-values))

    rows_copy.wait_recv()
    r.xs[0, slots:, :] = pick_rows(slot_table(1), 1, 0)
    pl.when(ep_of(3) < e)(spread_packs)
    spread_row = lax.broadcasted_iota(jnp.int32, (r.wq_t.shape[0], heads * LANES), 0)
    spread_col = lax.broadcasted_iota(jnp.int32, (r.wq_t.shape[0], heads * LANES), 1)
    in_head = spread_col % LANES
    spread = (
        (in_head < NOPE + ROPE_DIM)
        & (spread_row == (spread_col // LANES) * (NOPE + ROPE_DIM) + in_head)
    ).astype(f32).astype(bf16)
    r.wq[...] = lax.dot_general(
        r.wq_t[...], spread, (((0,), (0,)), ((), ())), preferred_element_type=f32
    ).astype(bf16)
    loads["q"].wait()

    def project(i, _):
        here = pl.ds(pl.multiple_of(i * tile, tile), tile)
        values = r.q_raw[here, :].astype(f32)
        scale = lax.rsqrt(jnp.mean(values * values, -1, keepdims=True) + norm_eps)
        normed = (values * scale * r.q_gain[...]).astype(bf16)
        projected = jnp.dot(normed, r.wq[...], preferred_element_type=f32)
        for head in range(heads):
            straight = projected[:, head * LANES : (head + 1) * LANES]
            r.q_all[head, here, :] = rotated(
                straight, r.cosine[here, :], r.sine[here, :]
            ).astype(bf16)
        return 0

    lax.fori_loop(0, 4, project, 0)

    lane_half = lax.broadcasted_iota(jnp.int32, (half, LANES), 1)

    def expand(k):
        for h in range(2):
            source = r.ropes[k, h].astype(f32)
            pieces = [
                pltpu.roll(source, (NOPE - ROPE_DIM * g) % LANES, 1) for g in range(4)
            ]
            turned = jnp.concatenate(pieces, 0)
            turned = jnp.where(
                (lane_half >= NOPE) & (lane_half < NOPE + ROPE_DIM), turned, 0.0
            )
            product = jnp.dot(
                r.kvs[k, h * half : (h + 1) * half, :], r.wkv[...], preferred_element_type=f32
            )
            start = pl.ds(pl.multiple_of(k * rows + h * half, half), half)
            for head in range(heads):
                pair = product[:, head * LANES : (head + 1) * LANES]
                r.k_all[head, start, :] = jnp.where(lane_half < NOPE, pair, turned).astype(bf16)
                r.v_all[head, start, :] = jnp.where(lane_half == 0, 1.0, pair).astype(bf16)

    def attend(queries, carry, start, size, masked):
        scored = [
            lax.dot_general(
                queries[head],
                r.k_all[head, pl.ds(start, size), :],
                (((1,), (1,)), ((), ())),
                preferred_element_type=f32,
            )
            for head in range(heads)
        ]
        result = []
        for head in range(heads):
            scores = scored[head]
            old_max, acc = carry[head]
            if masked is not None:
                row = lax.broadcasted_iota(jnp.int32, scores.shape, 0) + masked
                column = lax.broadcasted_iota(jnp.int32, scores.shape, 1)
                scores = jnp.where(column <= row, scores, -jnp.inf)
            new_max = jnp.maximum(old_max, jnp.max(scores, -1, keepdims=True))
            weights = jnp.exp2((scores - new_max) * factor).astype(bf16)
            product = jnp.dot(
                weights, r.v_all[head, pl.ds(start, size), :], preferred_element_type=f32
            )
            result.append((new_max, acc * jnp.exp2((old_max - new_max) * factor) + product))
        return tuple(result)

    expand(0)

    for i in range(4):
        here = slice(i * tile, (i + 1) * tile)
        queries = [r.q_all[head, here, :] for head in range(heads)]
        carry = tuple(
            (jnp.full((tile, 1), floor_value, f32), jnp.zeros((tile, LANES), f32))
            for head in range(heads)
        )
        carry = attend(queries, carry, 0, (i + 1) * tile, i * tile)
        for head in range(heads):
            r.top[head, here, :] = jnp.broadcast_to(carry[head][0], (tile, LANES))
            r.acc[head, here, :] = carry[head][1]

    for k in (1, 2):

        @pl.when(ep_of(k) < e)
        def _(k=k):
            for copy, forward in zip(pack_copies(k), pack_forwards(k)):
                copy.wait_recv()
                forward.start()

    for k in (1, 2):

        @pl.when(ep_of(k) < e)
        def _(k=k):
            for forward in pack_forwards(k):
                forward.wait_recv()
            expand(k)

    head_cols = heads * VDIM
    own_cols = pl.ds(pl.multiple_of(t * head_cols, head_cols), head_cols)

    wide = rows // 2
    outer = 1 - ((d + 1) // 2) % 2
    z_pair = d + 1 - 2 * (d % 2)
    z_cross = outer * (3 - z_pair) + (1 - outer) * (3 - d)

    def head_copy(i, j):
        device = (partner, (e, z_pair * 2 + c), (e, z_cross * 2 + c))[j]
        here = pl.ds(pl.multiple_of(i * wide, wide), wide)
        return remote(
            r.mixers.at[here, own_cols], r.mixers.at[here, own_cols],
            r.h_s.at[i, j], r.h_r.at[i, j + outer if j == 2 else j], device,
        )

    def head_cross(i, j):
        here = pl.ds(pl.multiple_of(i * wide, wide), wide)
        return remote(
            r.mixers.at[here, own_cols], r.mixers.at[here, own_cols],
            r.h_s.at[i, 2], r.h_r.at[i, 2 + j], (e, z_cross * 2 + c),
        )

    def head_relay(i, j):
        source = ((3 - d, (9 - 3 * (d + 1)) % 4)[j]) * 2 + c
        here = pl.ds(pl.multiple_of(i * wide, wide), wide)
        cols = pl.ds(pl.multiple_of(source * head_cols, head_cols), head_cols)
        return remote(
            r.mixers.at[here, cols], r.mixers.at[here, cols],
            r.h_s.at[i, 3 + j], r.h_r.at[i, 4 + j], (e, z_pair * 2 + c),
        )

    def relay_heads(first, last):
        @pl.when(outer == 0)
        def _():
            for i in range(first, last):
                for j in range(2):
                    head_cross(i, j).wait_recv()
                    head_relay(i, j).start()

    def head_forward(j):
        source = ((d + depths - j) % depths) * 2 + c
        cols = pl.ds(pl.multiple_of(source * head_cols, head_cols), head_cols)
        return remote(
            r.mixers.at[:, cols], r.mixers.at[:, cols],
            r.hf_s.at[j - 1], r.hf_r.at[j - 1], partner,
        )

    near_first = 1 + ey * (1 - ex)
    near_count = (ex + ey + 1) // 2 + ex * ey
    far_count = ey

    def tile_state(i):
        here = pl.ds(pl.multiple_of(i * wide, wide), wide)
        queries = [r.q_all[head, here, :] for head in range(heads)]
        carry = tuple(
            (r.top[head, here, :][:, :1], r.acc[head, here, :]) for head in range(heads)
        )
        return here, queries, carry

    def forward_far():
        for j in range(1, depths):
            for copy in pack_spreads(j):
                copy.wait_recv()
        for forward in pack_forwards(3):
            forward.start()

    def near_tile(i, _):
        here, queries, carry = tile_state(i)
        carry = lax.fori_loop(
            0, near_count,
            lambda s, cc: attend(
                queries, cc, pl.multiple_of((near_first + s) * rows, rows), rows, None
            ),
            carry,
        )
        for head in range(heads):
            r.top[head, here, :] = jnp.broadcast_to(carry[head][0], (wide, LANES))
            r.acc[head, here, :] = carry[head][1]

        pl.when((i == 0) & (ep_of(3) < e))(forward_far)
        return 0

    spread_slots()
    lax.fori_loop(0, 2, near_tile, 0)

    @pl.when(ep_of(3) < e)
    def _():
        for forward in pack_forwards(3):
            forward.wait_recv()
        expand(3)

    def far_tile(i, _):
        here, queries, carry = tile_state(i)
        carry = lax.fori_loop(
            0, far_count,
            lambda s, cc: attend(queries, cc, 3 * rows, rows, None),
            carry,
        )
        outs = [acc[:, NOPE : NOPE + VDIM] / acc[:, :1] for _, acc in carry]
        r.mixers[here, own_cols] = jnp.concatenate(outs, -1).astype(bf16)
        for j in (2, 1, 0):
            head_copy(i, j).start()
        return 0

    lax.fori_loop(0, 2, far_tile, 0)

    for k in (1, 2, 3):
        if k == 3:
            for j in range(1, depths):
                slot_spread(j).wait_recv()
        else:
            slot_sends(k).wait_recv()
        slot_forward(k).start()
    for name in ("eg", "eu", "ed"):
        loads[name].wait()

    quarter = width // 4
    chunks = [(n * quarter, quarter) for n in range(4)]

    def partial_copy(n, k):
        cols = pl.ds(*chunks[n])
        at = (k if n == 0 else slice(None), slice(None), cols)
        return remote(
            r.theirs.at[at], r.pair.at[at],
            r.ex_s.at[n, k if n == 0 else 0], r.ex_r.at[n, k if n == 0 else 0], partner,
        )

    def return_copy(n, k):
        cols = pl.ds(*chunks[n])
        return remote(
            r.sums.at[k, pl.ds(0, slots), cols], r.back.at[k, pl.ds(0, slots), cols],
            r.rt_s.at[n, k - 1], r.rt_r.at[n, k - 1], (ep_of(k), t),
        )

    hidden_units = r.eg.shape[1]
    step = min(256, hidden_units)

    def expert_hidden(k):
        inputs = r.xs[k]
        for n in range(0, hidden_units, step):
            gate = silu(jnp.dot(inputs, r.eg[:, n : n + step], preferred_element_type=f32))
            up = jnp.dot(inputs, r.eu[:, n : n + step], preferred_element_type=f32)
            r.hid[k, :, n : n + step] = (gate * up).astype(bf16)

    def expert_down(n, k):
        for start in range(chunks[n][0], sum(chunks[n]), quarter):
            cols = slice(start, start + quarter)
            product = jnp.dot(
                r.hid[k], r.ed[:, cols], preferred_element_type=f32
            ).astype(bf16)
            r.ours[k, :, cols] = product[:slots]
            r.theirs[k, :, cols] = product[slots:]

    def add_pair(n, k):
        cols = slice(chunks[n][0], sum(chunks[n]))
        r.sums[k, :slots, cols] = (
            r.ours[k, :, cols].astype(f32) + r.pair[k, :, cols].astype(f32)
        ).astype(bf16)

    def first_pass(i, _):
        k = (i + 1) % 4

        @pl.when(k > 0)
        def _():
            slot_forward(k).wait_recv()

        expert_hidden(k)
        expert_down(0, k)
        partial_copy(0, k).start()

        @pl.when(i > 0)
        def _():
            partial_copy(0, i).wait_recv()
            add_pair(0, i)
            return_copy(0, i).start()

        pl.when(i == 2)(lambda: relay_heads(0, 1))
        return 0

    r.back[:, slots:, :] = jnp.zeros((4, r.back.shape[1] - slots, width), bf16)
    r.sums[0, slots:, :] = jnp.zeros((r.back.shape[1] - slots, width), bf16)
    lax.fori_loop(0, 4, first_pass, 0)

    def later_pass(n):
        def one(k, _):
            expert_down(n, k)
            return 0

        lax.fori_loop(0, 4, one, 0)
        partial_copy(n, 0).start()

    def later_sums(n):
        partial_copy(n, 0).wait_recv()

        def one(k, _):
            add_pair(n, k)
            return_copy(n, k).start()
            return 0

        lax.fori_loop(1, 4, one, 0)
        add_pair(n, 0)

    later_pass(1)
    partial_copy(0, 0).wait_recv()
    add_pair(0, 0)
    later_pass(2)
    later_sums(1)
    relay_heads(1, 2)
    later_pass(3)
    later_sums(2)
    later_sums(3)
    for name in ("sg", "su", "sd"):
        loads[name].wait()
    for q in range(2):
        inputs = r.nrm[q]
        hidden = silu(jnp.dot(inputs, r.sg[...], preferred_element_type=f32))
        hidden = (hidden * jnp.dot(inputs, r.su[...], preferred_element_type=f32)).astype(bf16)
        r.shared[q] = jnp.dot(hidden, r.sd[...], preferred_element_type=f32).astype(bf16)
    shared_copy = remote(r.shared.at[1], r.shared.at[2], r.sh_s, r.sh_r, partner)
    shared_copy.start()

    shared_copy.wait_recv()

    tags = gather_rows(0)
    routes, weight = tags[:, :top], tags[:, top : 2 * top]
    factors = [
        jnp.sum(
            jnp.where(routes == ep_of(k).astype(f32), weight, 0.0), -1, keepdims=True
        )
        for k in range(4)
    ]

    def z_copy(n, j):
        there = depth_of(j)
        cols = pl.ds(*chunks[n])
        return remote(
            r.zs.at[pl.ds(pl.multiple_of(there * MOE_DEV, MOE_DEV), MOE_DEV), cols],
            r.zr.at[j - 1, :, cols],
            r.z_s.at[n, j - 1], r.z_r.at[n, j - 1], (e, there * 2 + c),
        )

    def combine(n):
        for k in (3, 2, 1):
            return_copy(n, k).wait_recv()
        for start in range(chunks[n][0], sum(chunks[n]), quarter):
            cols = slice(start, start + quarter)
            total = r.shared[0, :, cols].astype(f32) + r.shared[2, :, cols].astype(f32)
            for k in range(4):
                source = r.back if k > 0 else r.sums
                total = total + factors[k] * jnp.dot(
                    r.onehot[k], source[k, :, cols], preferred_element_type=f32
                )
            r.zs[:, cols] = total.astype(bf16)
        for j in range(1, depths):
            z_copy(n, j).start()

    def mix(i, _):
        here = pl.ds(pl.multiple_of(i * tile, tile), tile)
        r.mixed[here, :] = jnp.dot(
            r.mixers[here, :], r.wo[...], preferred_element_type=f32
        ).astype(bf16)
        return 0

    combine(0)
    combine(1)
    combine(2)
    for i in range(2):
        head_copy(i, 1).wait_recv()

    @pl.when(outer == 1)
    def _():
        for i in range(2):
            for j in range(2):
                head_relay(i, j).wait_recv()

    for j in range(1, depths):
        head_forward(j).start()
    combine(3)
    loads["wo"].wait()
    for i in range(2):
        head_copy(i, 0).wait_recv()
    for j in range(1, depths):
        head_forward(j).wait_recv()
    lax.fori_loop(0, 4, mix, 0)
    for n in range(len(chunks)):
        for j in range(1, depths):
            z_copy(n, j).wait_recv()
    final = r.zs[pl.ds(pl.multiple_of(d * MOE_DEV, MOE_DEV), MOE_DEV), :].astype(f32)
    for j in range(1, depths):
        final = final + r.zr[j - 1].astype(f32)
    r.moe_out[...] = final.astype(bf16)

    for k in (1, 2, 3):

        @pl.when(ep_of(k) > e)
        def _(k=k):
            for copy in pack_copies(k):
                copy.wait_send()

        @pl.when(ep_of(k) < e)
        def _(k=k):
            for copy in pack_forwards(k):
                copy.wait_send()
            if k == 3:
                for j in range(1, depths):
                    for copy in pack_spreads(j):
                        copy.wait_send()

        slot_sends(k).wait_send()
        slot_forward(k).wait_send()
        for n in range(len(chunks)):
            return_copy(n, k).wait_send()
    shared_copy.wait_send()
    rows_copy.wait_send()
    for k in range(4):
        partial_copy(0, k).wait_send()
    for n in range(1, len(chunks)):
        partial_copy(n, 0).wait_send()
    for i in range(2):
        for j in range(3):
            head_copy(i, j).wait_send()

    @pl.when(outer == 0)
    def _():
        for i in range(2):
            for j in range(2):
                head_relay(i, j).wait_send()

    for j in range(1, depths):
        slot_spread(j).wait_send()
        head_forward(j).wait_send()
        for n in range(len(chunks)):
            z_copy(n, j).wait_send()


def rotary_constant(total, per_device):
    halfway = ROPE_DIM // 2
    inverse = (
        np.float32(rotary_base)
        ** (-(np.arange(halfway, dtype=np.float32) * np.float32(2.0) / np.float32(ROPE_DIM)))
    ).astype(np.float32)
    angles = (np.arange(total, dtype=np.float32)[:, None] * inverse[None, :]).astype(np.float32)
    angles = angles.astype(np.float64)
    both = np.concatenate([np.cos(angles), np.sin(angles)], 1).astype(np.float32)
    groups = both.reshape(-1, LANES // ROPE_DIM, per_device * ROPE_DIM // LANES, ROPE_DIM)
    return groups.transpose(0, 2, 1, 3).reshape(-1, LANES)


def fused_body(
    q_latent,
    kv_latent,
    rope_key,
    q_gain,
    kv_gain,
    w_query,
    w_keyval,
    w_output,
    moe_input,
    moe_gain,
    routes,
    route_weight,
    expert_gate,
    expert_up,
    expert_down,
    shared_gate,
    shared_up,
    shared_down,
):
    rows, qlat = q_latent.shape
    latent = kv_latent.shape[1]
    ep_count = lax.axis_size("ep")
    tp_count = lax.axis_size("tp")
    heads = w_query.shape[1] // (NOPE + ROPE_DIM)
    tokens, width = moe_input.shape
    side = tokens // 2
    depths = tp_count // 2
    hidden = expert_gate.shape[2]
    shared_hidden = shared_gate.shape[1]
    top = routes.shape[1]
    capacity = 3 * MOE_DEV * top // (2 * ep_count)
    slots = depths * capacity
    columns = w_output.shape[1]
    bf16, f32 = jnp.bfloat16, jnp.float32
    table = jnp.asarray(rotary_constant(rows * ep_count, rows))
    hbm = pl.BlockSpec(memory_space=pltpu.HBM)
    vmem = pl.BlockSpec(memory_space=pltpu.VMEM)
    inputs = [
        ("q_hbm", q_latent, hbm),
        ("kv_hbm", kv_latent, hbm),
        ("table_hbm", table, hbm),
        ("moe_hbm", moe_input, hbm),
        ("eg_hbm", expert_gate, hbm),
        ("eu_hbm", expert_up, hbm),
        ("ed_hbm", expert_down, hbm),
        ("sg_hbm", shared_gate, hbm),
        ("su_hbm", shared_up, hbm),
        ("sd_hbm", shared_down, hbm),
        ("wo_hbm", w_output, hbm),
        ("rope_t", rope_key.T, vmem),
        ("q_gain", q_gain.reshape(1, -1), vmem),
        ("kv_gain", kv_gain.reshape(1, -1), vmem),
        ("wq_t", w_query.T, vmem),
        ("wkv", w_keyval, vmem),
        ("moe_gain", moe_gain.reshape(1, -1), vmem),
        ("routes_t", routes.T, vmem),
        ("weight_t", route_weight.T, vmem),
    ]
    outputs = [("mixed", (rows, columns)), ("moe_out", (MOE_DEV, width))]
    dma = pltpu.SemaphoreType.DMA
    scratch = [
        ("kv_raw", pltpu.VMEM((rows, latent), bf16)),
        ("q_raw", pltpu.VMEM((rows, qlat), bf16)),
        ("table", pltpu.VMEM((rows // 4, LANES), f32)),
        ("tags", pltpu.VMEM((LANES, tokens), f32)),
        ("tagged", pltpu.VMEM((tokens, LANES), f32)),
        ("wq", pltpu.VMEM((qlat, heads * LANES), bf16)),
        ("cosine", pltpu.VMEM((rows, LANES), f32)),
        ("sine", pltpu.VMEM((rows, LANES), f32)),
        ("kvs", pltpu.VMEM((4, rows, latent), bf16)),
        ("ropes", pltpu.VMEM((4, 2, rows // 8, LANES), bf16)),
        ("nrm", pltpu.VMEM((2, side, width), bf16)),
        ("onehot", pltpu.VMEM((4, side, LANES), bf16)),
        ("snd", pltpu.VMEM((3, slots, width), bf16)),
        ("xs", pltpu.VMEM((4, 2 * slots, width), bf16)),
        ("shared", pltpu.VMEM((3, side, width), bf16)),
        ("q_all", pltpu.VMEM((heads, rows, LANES), bf16)),
        ("k_all", pltpu.VMEM((heads, 4 * rows, LANES), bf16)),
        ("v_all", pltpu.VMEM((heads, 4 * rows, LANES), bf16)),
        ("top", pltpu.VMEM((heads, rows, LANES), f32)),
        ("acc", pltpu.VMEM((heads, rows, LANES), f32)),
        ("mixers", pltpu.VMEM((rows, tp_count * heads * VDIM), bf16)),
        ("ours", pltpu.VMEM((4, slots, width), bf16)),
        ("theirs", pltpu.VMEM((4, slots, width), bf16)),
        ("pair", pltpu.VMEM((4, slots, width), bf16)),
        ("sums", pltpu.VMEM((4, LANES, width), bf16)),
        ("hid", pltpu.VMEM((4, 2 * slots, hidden), bf16)),
        ("back", pltpu.VMEM((4, LANES, width), bf16)),
        ("zs", pltpu.VMEM((side, width), bf16)),
        ("zr", pltpu.VMEM((depths - 1, MOE_DEV, width), bf16)),
        ("eg", pltpu.VMEM((width, hidden), bf16)),
        ("eu", pltpu.VMEM((width, hidden), bf16)),
        ("ed", pltpu.VMEM((hidden, width), bf16)),
        ("sg", pltpu.VMEM((width, shared_hidden), bf16)),
        ("su", pltpu.VMEM((width, shared_hidden), bf16)),
        ("sd", pltpu.VMEM((shared_hidden, width), bf16)),
        ("wo", pltpu.VMEM(w_output.shape, bf16)),
        ("ld", dma((10 + depths,))),
        ("pk_s", dma((3, 2))),
        ("pk_r", dma((3, 2))),
        ("pf_s", dma((3, 2))),
        ("pf_r", dma((3, 2))),
        ("sl_s", dma((3,))),
        ("sl_r", dma((3,))),
        ("ps_s", dma((depths - 1, 2))),
        ("ps_r", dma((depths - 1, 2))),
        ("ss_s", dma((depths - 1,))),
        ("ss_r", dma((depths - 1,))),
        ("sf_s", dma((3,))),
        ("sf_r", dma((3,))),
        ("rc_s", dma),
        ("rc_r", dma),
        ("sh_s", dma),
        ("sh_r", dma),
        ("ex_s", dma((4, 4))),
        ("ex_r", dma((4, 4))),
        ("rt_s", dma((4, 3))),
        ("rt_r", dma((4, 3))),
        ("h_s", dma((2, 5))),
        ("h_r", dma((2, 6))),
        ("hf_s", dma((depths - 1,))),
        ("hf_r", dma((depths - 1,))),
        ("z_s", dma((4, depths - 1))),
        ("z_r", dma((4, depths - 1))),
    ]
    names = [x[0] for x in inputs] + [x[0] for x in outputs] + [x[0] for x in scratch]
    mixed, moe_out = pl.pallas_call(
        lambda *refs: fused_kernel(names, *refs),
        out_shape=[jax.ShapeDtypeStruct(shape, bf16) for _, shape in outputs],
        in_specs=[spec for _, _, spec in inputs],
        out_specs=[vmem] * len(outputs),
        scratch_shapes=[spec for _, spec in scratch],
        compiler_params=pltpu.CompilerParams(
            collective_id=0,
            has_side_effects=True,
            vmem_limit_bytes=60 * 1024 * 1024,
        ),
        name="fused",
    )(*[value for _, value, _ in inputs])
    return (mixed, moe_out)


def solution(mesh):
    in_specs = (
        P("ep", None),
        P("ep", None),
        P("ep", None),
        P(),
        P(),
        P(None, "tp"),
        P(None, "tp"),
        P(None, "tp"),
        P("ep", None),
        P(),
        P("ep", None),
        P("ep", None),
        P("ep", None, "tp"),
        P("ep", None, "tp"),
        P("ep", "tp", None),
        P(None, "tp"),
        P(None, "tp"),
        P("tp", None),
    )
    out_specs = (P("ep", "tp"), P(("ep", "tp"), None))
    chosen = fused_body if (mesh.shape["ep"], mesh.shape["tp"]) == (4, 8) else body
    return jax.shard_map(
        chosen, mesh=mesh, in_specs=in_specs, out_specs=out_specs, check_vma=False
    )
```

```python
import jax
import jax.numpy as jnp
import numpy as np
from jax import lax
from jax.experimental import pallas as pl
from jax.experimental.pallas import tpu as pltpu
from jax.sharding import PartitionSpec as P

NOPE = 64
ROPE_DIM = 32
VDIM = 64
MOE_DEV = 32


norm_eps = 1e-06
layer_eps = 1e-05
rotary_base = 10000.0
floor_value = -1e30


def rms_scale(values, gain):
    widened = values.astype(jnp.float32)
    return (
        widened * lax.rsqrt(jnp.mean(widened * widened, -1, keepdims=True) + norm_eps) * gain
    ).astype(jnp.bfloat16)


def layer_scale(values, gain):
    widened = values.astype(jnp.float32)
    centred = widened - jnp.mean(widened, -1, keepdims=True)
    return (
        centred * lax.rsqrt(jnp.mean(centred * centred, -1, keepdims=True) + layer_eps) * gain
    ).astype(jnp.bfloat16)


def rotary_tables(positions):
    halfway = ROPE_DIM // 2
    inverse = rotary_base ** (-(jnp.arange(halfway, dtype=jnp.float32) * 2.0 / ROPE_DIM))
    angles = positions.astype(jnp.float32)[:, None] * inverse[None, :]
    return (jnp.cos(angles), jnp.sin(angles))


def rotate(values, cosine_table, sine_table):
    halfway = values.shape[-1] // 2
    first_half = values[..., :halfway]
    second_half = values[..., halfway:]
    return jnp.concatenate(
        [
            first_half * cosine_table - second_half * sine_table,
            second_half * cosine_table + first_half * sine_table,
        ],
        -1,
    )


def block_stats(query_block, query_pos, keyvals, rotated_keys, key_pos):
    scale = float(NOPE + ROPE_DIM) ** (-0.5)
    scores = jnp.einsum(
        "qhd,khd->hqk",
        query_block[..., :NOPE],
        keyvals[..., :NOPE],
        preferred_element_type=jnp.float32,
    )
    scores = (
        scores
        + jnp.einsum(
            "qhd,kd->hqk", query_block[..., NOPE:], rotated_keys, preferred_element_type=jnp.float32
        )
    ) * scale
    allowed = key_pos[None, :] <= query_pos[:, None]
    scores = jnp.where(allowed[None], scores, -jnp.inf)
    block_max = jnp.max(scores, -1)
    weights = jnp.exp(scores - block_max[..., None])
    block_sum = jnp.sum(weights, -1)
    attended = jnp.einsum(
        "hqk,khd->qhd",
        weights.astype(jnp.bfloat16),
        keyvals[..., NOPE:],
        preferred_element_type=jnp.float32,
    ).astype(jnp.bfloat16)
    return (block_max.T, block_sum.T, attended)


def merge_block(carried, stats):
    running_max, running_sum, running_acc = carried
    block_max, block_sum, attended = stats
    new_max = jnp.maximum(running_max, block_max)
    old_weight = jnp.exp(running_max - new_max)
    new_weight = jnp.exp(block_max - new_max)
    return (
        new_max,
        running_sum * old_weight + block_sum * new_weight,
        running_acc * old_weight[..., None] + attended.astype(jnp.float32) * new_weight[..., None],
    )


def body(
    q_latent,
    kv_latent,
    rope_key,
    q_gain,
    kv_gain,
    w_query,
    w_keyval,
    w_output,
    moe_input,
    moe_gain,
    routes,
    route_weight,
    expert_gate,
    expert_up,
    expert_down,
    shared_gate,
    shared_up,
    shared_down,
):
    row_count = q_latent.shape[0]
    own_index = lax.axis_index("ep")
    ep_count = lax.axis_size("ep")
    tp_count = lax.axis_size("tp")
    positions = own_index * row_count + jnp.arange(row_count, dtype=jnp.int32)
    cosine_table, sine_table = rotary_tables(positions)
    q_normed = rms_scale(q_latent, q_gain)
    kv_normed = rms_scale(kv_latent, kv_gain)
    key_rotated = rotate(rope_key.astype(jnp.float32), cosine_table, sine_table).astype(
        jnp.bfloat16
    )
    heads_local = w_query.shape[1] // (NOPE + ROPE_DIM)
    projected = jnp.dot(q_normed, w_query, preferred_element_type=jnp.float32)
    projected = projected.reshape(row_count, heads_local, NOPE + ROPE_DIM)
    queries = jnp.concatenate(
        [
            projected[..., :NOPE],
            rotate(projected[..., NOPE:], cosine_table[:, None, :], sine_table[:, None, :]),
        ],
        -1,
    ).astype(jnp.bfloat16)

    def expand_keys(latent_rows):
        expanded = jnp.dot(latent_rows, w_keyval, preferred_element_type=jnp.float32).astype(
            jnp.bfloat16
        )
        return expanded.reshape(latent_rows.shape[0], heads_local, NOPE + VDIM)

    initial = (
        jnp.full((row_count, heads_local), floor_value, jnp.float32),
        jnp.zeros((row_count, heads_local), jnp.float32),
        jnp.zeros((row_count, heads_local, VDIM), jnp.float32),
    )
    carried = initial
    latent_piece = lax.all_gather(kv_normed, "ep", axis=0, tiled=True)
    rotated_piece = lax.all_gather(key_rotated, "ep", axis=0, tiled=True)
    block_count = latent_piece.shape[0] // row_count

    def visit_block(inner, offset):

        def live(current):
            latent_rows = lax.dynamic_slice_in_dim(latent_piece, offset * row_count, row_count, 0)
            rotated_rows = lax.dynamic_slice_in_dim(rotated_piece, offset * row_count, row_count, 0)
            key_pos = offset * row_count + jnp.arange(row_count, dtype=jnp.int32)
            stats = block_stats(queries, positions, expand_keys(latent_rows), rotated_rows, key_pos)
            return merge_block(current, stats)

        def skipped(current):
            return current

        return (lax.cond(offset <= own_index, live, skipped, inner), None)

    carried, unused = lax.scan(visit_block, carried, jnp.arange(block_count, dtype=jnp.int32))
    running_max, running_sum, running_acc = carried
    heads_out = (
        (running_acc / running_sum[..., None])
        .astype(jnp.bfloat16)
        .reshape(row_count, heads_local * VDIM)
    )
    mixed = jnp.dot(
        lax.all_gather(heads_out, "tp", axis=1, tiled=True),
        w_output,
        preferred_element_type=jnp.float32,
    )
    mixed = mixed.astype(jnp.bfloat16)
    width = moe_input.shape[1]
    top_count = routes.shape[1]
    local_experts = expert_gate.shape[0]
    expert_count = local_experts * ep_count
    capacity = max(2, 3 * MOE_DEV * top_count // (2 * expert_count))
    normed = layer_scale(moe_input, moe_gain)
    entries = routes.reshape(tp_count, MOE_DEV * top_count)
    onehot = (entries[..., None] == jnp.arange(expert_count, dtype=jnp.int32)).astype(jnp.int32)
    earlier = jnp.cumsum(onehot, 1) - onehot
    rank_in = jnp.sum(earlier * onehot, -1)
    block_ids = jnp.arange(tp_count, dtype=jnp.int32)[:, None]
    slot_of = ((entries * tp_count + block_ids) * capacity + rank_in).reshape(-1, top_count)
    token_ids = jnp.arange(tp_count * MOE_DEV * top_count, dtype=jnp.int32) // top_count
    slot_token = (
        jnp.full((expert_count * tp_count * capacity,), -1, jnp.int32)
        .at[slot_of.reshape(-1)]
        .set(token_ids)
    )
    outgoing = jnp.where(
        (slot_token >= 0)[:, None], normed[jnp.maximum(slot_token, 0)], jnp.zeros((), jnp.bfloat16)
    )
    outgoing = outgoing.reshape(ep_count, local_experts, tp_count, capacity, width)
    arrived = lax.all_to_all(outgoing, "ep", split_axis=0, concat_axis=0, tiled=True)
    slot_rows = arrived.shape[3]
    inputs = arrived[:, 0].reshape(-1, width)
    hidden = jax.nn.silu(jnp.dot(inputs, expert_gate[0], preferred_element_type=jnp.float32))
    hidden = (hidden * jnp.dot(inputs, expert_up[0], preferred_element_type=jnp.float32)).astype(
        jnp.bfloat16
    )
    output = jnp.dot(hidden, expert_down[0], preferred_element_type=jnp.float32)
    results = [output.astype(jnp.bfloat16).reshape(ep_count, tp_count, slot_rows, width)]
    partial_value = jnp.stack(results, 1)
    shared_hidden = jax.nn.silu(jnp.dot(normed, shared_gate, preferred_element_type=jnp.float32))
    shared_hidden = (
        shared_hidden * jnp.dot(normed, shared_up, preferred_element_type=jnp.float32)
    ).astype(jnp.bfloat16)
    shared_part = jnp.dot(shared_hidden, shared_down, preferred_element_type=jnp.float32).astype(
        jnp.bfloat16
    )
    slot_total, shared_total = (
        lax.psum_scatter(
            partial_value.astype(jnp.float32).astype(jnp.bfloat16),
            "tp",
            scatter_dimension=2,
            tiled=True,
        ).astype(jnp.float32),
        lax.psum_scatter(
            shared_part.astype(jnp.float32)
            .reshape(1, 1, tp_count, MOE_DEV, width)
            .astype(jnp.bfloat16),
            "tp",
            scatter_dimension=2,
            tiled=True,
        ).astype(jnp.float32),
    )
    arrived_sums = lax.all_to_all(
        slot_total.astype(jnp.bfloat16), "ep", split_axis=0, concat_axis=0, tiled=True
    ).astype(slot_total.dtype)
    own_block = lax.axis_index("tp")
    own_entries = lax.dynamic_slice_in_dim(routes, own_block * MOE_DEV, MOE_DEV, 0)
    own_rank = lax.dynamic_slice_in_dim(
        rank_in.reshape(-1, top_count), own_block * MOE_DEV, MOE_DEV, 0
    )
    own_weight = lax.dynamic_slice_in_dim(route_weight, own_block * MOE_DEV, MOE_DEV, 0)
    picked = arrived_sums.reshape(-1, width)[own_entries * capacity + own_rank]
    moe_out = (
        jnp.sum(own_weight[..., None] * picked, 1) + shared_total.reshape(MOE_DEV, width)
    ).astype(jnp.bfloat16)
    return (mixed, moe_out)


LANES = 128
LOG2E = 1.4426950408889634
MESH = pl.DeviceIdType.MESH


class Refs:
    pass


def fused_kernel(names, *refs):
    r = Refs()
    for name, ref in zip(names, refs):
        setattr(r, name, ref)
    f32, bf16 = jnp.float32, jnp.bfloat16
    e = lax.axis_index("ep")
    t = lax.axis_index("tp")
    c = t % 2
    d = t // 2
    ex, ey = e % 2, e // 2
    partner = (e, t + 1 - 2 * c)
    rows = r.kv_hbm.shape[0]
    half = rows // 2
    tile = rows // 4
    eighth = rows // 8
    latent = r.kv_hbm.shape[1]
    heads = r.k_all.shape[0]
    width = r.moe_hbm.shape[1]
    slots = r.xs.shape[1] // 2
    side = r.nrm.shape[1]
    depths = side // MOE_DEV
    capacity = slots // depths
    factor = float(NOPE + ROPE_DIM) ** (-0.5) * LOG2E
    halfway = ROPE_DIM // 2

    def ep_of(k):
        return ((ey + k // 2) % 2) * 2 + (ex + k % 2) % 2

    def rel_of(source):
        return ((source // 2 + ey) % 2) * 2 + (source % 2 + ex) % 2

    def remote(src, dst, send, recv, device):
        return pltpu.make_async_remote_copy(
            src_ref=src, dst_ref=dst, send_sem=send, recv_sem=recv,
            device_id=device, device_id_type=MESH,
        )

    loads = {}

    def load(name, src, dst, sem):
        copy = pltpu.make_async_copy(src, dst, r.ld.at[sem])
        copy.start()
        loads[name] = copy

    load("kv", r.kv_hbm, r.kv_raw, 0)
    load("table", r.table_hbm.at[pl.ds(pl.multiple_of(e * tile, tile), tile)], r.table, 1)
    for j in range(depths):
        load(
            f"moe{j}",
            r.moe_hbm.at[pl.ds(pl.multiple_of((2 * j + c) * MOE_DEV, MOE_DEV), MOE_DEV)],
            r.nrm.at[0, pl.ds(j * MOE_DEV, MOE_DEV)],
            2 + j,
        )
    first = 2 + depths
    load("q", r.q_hbm, r.q_raw, first)
    load("sg", r.sg_hbm, r.sg, first + 1)
    load("su", r.su_hbm, r.su, first + 2)
    load("sd", r.sd_hbm, r.sd, first + 3)
    load("eg", r.eg_hbm.at[0], r.eg, first + 4)
    load("eu", r.eu_hbm.at[0], r.eu, first + 5)
    load("ed", r.ed_hbm.at[0], r.ed, first + 6)
    load("wo", r.wo_hbm, r.wo, first + 7)

    barrier = pltpu.get_barrier_semaphore()
    peers = [partner] + [(ep_of(k), t) for k in (1, 2, 3)]
    peers += [(e, ((d + j) % depths) * 2 + c) for j in range(1, depths)]
    for peer in peers:
        pl.semaphore_signal(barrier, inc=1, device_id=peer, device_id_type=MESH)

    lane = lax.broadcasted_iota(jnp.int32, (tile, LANES), 1)
    low = (lane >= NOPE) & (lane < NOPE + halfway)
    high = (lane >= NOPE + halfway) & (lane < NOPE + ROPE_DIM)

    def rotated(values, cosine, sine):
        swapped = jnp.where(
            lane < NOPE + halfway,
            pltpu.roll(values, LANES - halfway, 1),
            pltpu.roll(values, halfway, 1),
        )
        return values * cosine + swapped * sine

    place = (
        lax.broadcasted_iota(jnp.int32, (ROPE_DIM, LANES), 0) + NOPE
        == lax.broadcasted_iota(jnp.int32, (ROPE_DIM, LANES), 1)
    ).astype(f32).astype(bf16)

    loads["table"].wait()
    loads["kv"].wait()

    def key_half(h):
        packed = jnp.zeros((eighth, LANES), f32)
        for which in range(2):
            i = 2 * h + which
            here = pl.ds(pl.multiple_of(i * tile, tile), tile)
            turned = pltpu.roll(r.table[...], (NOPE - ROPE_DIM * i + LANES) % LANES, 1)
            later = pltpu.roll(turned, halfway, 1)
            sooner = pltpu.roll(turned, LANES - halfway, 1)
            cosine = jnp.where(
                lane < NOPE, 1.0, jnp.where(low, turned, jnp.where(high, later, 0.0))
            )
            sine = jnp.where(low, -sooner, jnp.where(high, turned, 0.0))
            r.cosine[here, :] = cosine
            r.sine[here, :] = sine
            values = r.kv_raw[here, :].astype(f32)
            scale = lax.rsqrt(jnp.mean(values * values, -1, keepdims=True) + norm_eps)
            r.kvs[0, here, :] = (values * scale * r.kv_gain[...]).astype(bf16)
            straight = lax.dot_general(
                r.rope_t[:, here], place, (((0,), (0,)), ((), ())), preferred_element_type=f32
            )
            turned = rotated(straight, cosine, sine)
            for part in range(2):
                piece = turned[part * eighth : (part + 1) * eighth]
                shift = (ROPE_DIM * (2 * which + part) - NOPE) % LANES
                packed += pltpu.roll(piece, shift, 1)
        r.ropes[0, h] = packed.astype(bf16)

    key_half(c)
    pl.semaphore_wait(barrier, len(peers))

    own_half = pl.ds(pl.multiple_of(c * half, half), half)

    kv_part, rope_part = half // depths, eighth // depths

    def depth_of(j):
        return (d + j) % depths

    def z_peer(j):
        return (e, depth_of(j) * 2 + c)

    kv_quarter = pl.ds(pl.multiple_of(c * half + d * kv_part, kv_part), kv_part)
    rope_quarter = pl.ds(pl.multiple_of(d * rope_part, rope_part), rope_part)

    def pack_copies(k):
        device = (ep_of(k), t)
        kv_rows, rope_rows = (kv_quarter, rope_quarter) if k == 3 else (own_half, slice(None))
        return [
            remote(r.kvs.at[0, kv_rows], r.kvs.at[k, kv_rows],
                   r.pk_s.at[k - 1, 0], r.pk_r.at[k - 1, 0], device),
            remote(r.ropes.at[0, c, rope_rows], r.ropes.at[k, c, rope_rows],
                   r.pk_s.at[k - 1, 1], r.pk_r.at[k - 1, 1], device),
        ]

    def pack_spreads(j):
        return [
            remote(r.kvs.at[3, kv_quarter], r.kvs.at[3, kv_quarter],
                   r.ps_s.at[j - 1, 0], r.ps_r.at[j - 1, 0], z_peer(j)),
            remote(r.ropes.at[3, c, rope_quarter], r.ropes.at[3, c, rope_quarter],
                   r.ps_s.at[j - 1, 1], r.ps_r.at[j - 1, 1], z_peer(j)),
        ]

    def spread_packs():
        for copy in pack_copies(3):
            copy.wait_recv()
        for j in range(1, depths):
            for copy in pack_spreads(j):
                copy.start()

    def pack_forwards(k):
        return [
            remote(r.kvs.at[k, own_half], r.kvs.at[k, own_half],
                   r.pf_s.at[k - 1, 0], r.pf_r.at[k - 1, 0], partner),
            remote(r.ropes.at[k, c], r.ropes.at[k, c],
                   r.pf_s.at[k - 1, 1], r.pf_r.at[k - 1, 1], partner),
        ]

    for k in (3, 2, 1):

        @pl.when(ep_of(k) > e)
        def _(k=k):
            for copy in pack_copies(k):
                copy.start()

    key_half(1 - c)

    for j in range(depths):
        loads[f"moe{j}"].wait()

    chunk = 16

    def norm_rows(i, _):
        here = pl.ds(pl.multiple_of(i * chunk, chunk), chunk)
        values = r.nrm[0, here, :].astype(f32)
        centred = values - jnp.mean(values, -1, keepdims=True)
        scale = lax.rsqrt(jnp.mean(centred * centred, -1, keepdims=True) + layer_eps)
        r.nrm[0, here, :] = (centred * scale * r.moe_gain[...]).astype(bf16)
        return 0

    lax.fori_loop(0, side // chunk, norm_rows, 0, unroll=2)
    rows_copy = remote(r.nrm.at[0], r.nrm.at[1], r.rc_s, r.rc_r, partner)
    rows_copy.start()

    r.tags[...] = jnp.zeros(r.tags.shape, f32)
    top = r.routes_t.shape[0]
    r.tags[:top, :] = r.routes_t[...].astype(f32)
    r.tags[top : 2 * top, :] = r.weight_t[...]
    r.tagged[...] = r.tags[...].T

    row_id = lax.broadcasted_iota(jnp.int32, (side, side), 0)
    col_id = lax.broadcasted_iota(jnp.int32, (side, side), 1)
    earlier = (
        (col_id < row_id) & (col_id // MOE_DEV == row_id // MOE_DEV)
    ).astype(f32).astype(bf16)

    def gather_rows(q):
        return jnp.concatenate(
            [
                r.tagged[pl.ds(pl.multiple_of((2 * j + (c + q) % 2) * MOE_DEV, MOE_DEV), MOE_DEV), :]
                for j in range(depths)
            ],
            0,
        )

    lane_side = lax.broadcasted_iota(jnp.int32, (side, LANES), 1)
    block_of = lax.broadcasted_iota(jnp.int32, (side, LANES), 0) // MOE_DEV
    slot_cols = pl.ds(pl.multiple_of(d * (width // depths), width // depths), width // depths)

    def slot_sends(k):
        cols = slot_cols if k == 3 else slice(None)
        return remote(
            r.snd.at[k - 1, :, cols], r.xs.at[k, pl.ds(0, slots), cols],
            r.sl_s.at[k - 1], r.sl_r.at[k - 1], (ep_of(k), t),
        )

    def slot_spread(j):
        there = r.xs.at[3, pl.ds(0, slots), slot_cols]
        return remote(there, there, r.ss_s.at[j - 1], r.ss_r.at[j - 1], z_peer(j))

    def spread_slots():
        slot_sends(3).wait_recv()
        for j in range(1, depths):
            slot_spread(j).start()

    def slot_table(q):
        tags = gather_rows(q)
        named = lane_side < 0
        for k in range(top):
            named = named | (tags[:, k : k + 1] == lane_side.astype(f32))
        rank = jnp.dot(
            earlier, named.astype(f32).astype(bf16), preferred_element_type=f32
        )
        return jnp.where(named, rank + (block_of * capacity).astype(f32), -1.0)

    def pick_rows(slot, q, k):
        mine = jnp.sum(jnp.where(lane_side == ep_of(k), slot, 0.0), -1, keepdims=True)
        onehot = (mine == lane_side.astype(f32)).astype(f32)
        if q == 0:
            r.onehot[k] = onehot.astype(bf16)
        return jnp.dot(
            onehot.T.astype(bf16), r.nrm[q], preferred_element_type=f32
        )[:slots].astype(bf16)

    table = slot_table(0)
    for k in (3, 2, 1):
        r.snd[k - 1] = pick_rows(table, 0, k)
        slot_sends(k).start()
    r.xs[0, :slots, :] = pick_rows(table, 0, 0)

    def slot_forward(k):
        return remote(
            r.xs.at[k, pl.ds(0, slots)], r.xs.at[k, pl.ds(slots, slots)],
            r.sf_s.at[k - 1], r.sf_r.at[k - 1], partner,
        )

    def silu(values):
        return values / (1.0 + jnp.exp(-values))

    rows_copy.wait_recv()
    r.xs[0, slots:, :] = pick_rows(slot_table(1), 1, 0)
    pl.when(ep_of(3) < e)(spread_packs)
    spread_row = lax.broadcasted_iota(jnp.int32, (r.wq_t.shape[0], heads * LANES), 0)
    spread_col = lax.broadcasted_iota(jnp.int32, (r.wq_t.shape[0], heads * LANES), 1)
    in_head = spread_col % LANES
    spread = (
        (in_head < NOPE + ROPE_DIM)
        & (spread_row == (spread_col // LANES) * (NOPE + ROPE_DIM) + in_head)
    ).astype(f32).astype(bf16)
    r.wq[...] = lax.dot_general(
        r.wq_t[...], spread, (((0,), (0,)), ((), ())), preferred_element_type=f32
    ).astype(bf16)
    loads["q"].wait()

    def project(i, _):
        here = pl.ds(pl.multiple_of(i * tile, tile), tile)
        values = r.q_raw[here, :].astype(f32)
        scale = lax.rsqrt(jnp.mean(values * values, -1, keepdims=True) + norm_eps)
        normed = (values * scale * r.q_gain[...]).astype(bf16)
        projected = jnp.dot(normed, r.wq[...], preferred_element_type=f32)
        for head in range(heads):
            straight = projected[:, head * LANES : (head + 1) * LANES]
            r.q_all[head, here, :] = rotated(
                straight, r.cosine[here, :], r.sine[here, :]
            ).astype(bf16)
        return 0

    lax.fori_loop(0, 4, project, 0)

    lane_half = lax.broadcasted_iota(jnp.int32, (half, LANES), 1)

    def expand(k):
        for h in range(2):
            source = r.ropes[k, h].astype(f32)
            pieces = [
                pltpu.roll(source, (NOPE - ROPE_DIM * g) % LANES, 1) for g in range(4)
            ]
            turned = jnp.concatenate(pieces, 0)
            turned = jnp.where(
                (lane_half >= NOPE) & (lane_half < NOPE + ROPE_DIM), turned, 0.0
            )
            product = jnp.dot(
                r.kvs[k, h * half : (h + 1) * half, :], r.wkv[...], preferred_element_type=f32
            )
            start = pl.ds(pl.multiple_of(k * rows + h * half, half), half)
            for head in range(heads):
                pair = product[:, head * LANES : (head + 1) * LANES]
                r.k_all[head, start, :] = jnp.where(lane_half < NOPE, pair, turned).astype(bf16)
                r.v_all[head, start, :] = jnp.where(lane_half == 0, 1.0, pair).astype(bf16)

    def attend(queries, carry, start, size, masked):
        scored = [
            lax.dot_general(
                queries[head],
                r.k_all[head, pl.ds(start, size), :],
                (((1,), (1,)), ((), ())),
                preferred_element_type=f32,
            )
            for head in range(heads)
        ]
        result = []
        for head in range(heads):
            scores = scored[head]
            old_max, acc = carry[head]
            if masked is not None:
                row = lax.broadcasted_iota(jnp.int32, scores.shape, 0) + masked
                column = lax.broadcasted_iota(jnp.int32, scores.shape, 1)
                scores = jnp.where(column <= row, scores, -jnp.inf)
            new_max = jnp.maximum(old_max, jnp.max(scores, -1, keepdims=True))
            weights = jnp.exp2((scores - new_max) * factor).astype(bf16)
            product = jnp.dot(
                weights, r.v_all[head, pl.ds(start, size), :], preferred_element_type=f32
            )
            result.append((new_max, acc * jnp.exp2((old_max - new_max) * factor) + product))
        return tuple(result)

    expand(0)

    for i in range(4):
        here = slice(i * tile, (i + 1) * tile)
        queries = [r.q_all[head, here, :] for head in range(heads)]
        carry = tuple(
            (jnp.full((tile, 1), floor_value, f32), jnp.zeros((tile, LANES), f32))
            for head in range(heads)
        )
        carry = attend(queries, carry, 0, (i + 1) * tile, i * tile)
        for head in range(heads):
            r.top[head, here, :] = jnp.broadcast_to(carry[head][0], (tile, LANES))
            r.acc[head, here, :] = carry[head][1]

    for k in (1, 2):

        @pl.when(ep_of(k) < e)
        def _(k=k):
            for copy, forward in zip(pack_copies(k), pack_forwards(k)):
                copy.wait_recv()
                forward.start()

    for k in (1, 2):

        @pl.when(ep_of(k) < e)
        def _(k=k):
            for forward in pack_forwards(k):
                forward.wait_recv()
            expand(k)

    head_cols = heads * VDIM
    own_cols = pl.ds(pl.multiple_of(t * head_cols, head_cols), head_cols)

    wide = rows // 2
    outer = 1 - ((d + 1) // 2) % 2
    z_pair = d + 1 - 2 * (d % 2)
    z_cross = outer * (3 - z_pair) + (1 - outer) * (3 - d)

    def head_copy(i, j):
        device = (partner, (e, z_pair * 2 + c), (e, z_cross * 2 + c))[j]
        here = pl.ds(pl.multiple_of(i * wide, wide), wide)
        return remote(
            r.mixers.at[here, own_cols], r.mixers.at[here, own_cols],
            r.h_s.at[i, j], r.h_r.at[i, j + outer if j == 2 else j], device,
        )

    def head_cross(i, j):
        here = pl.ds(pl.multiple_of(i * wide, wide), wide)
        return remote(
            r.mixers.at[here, own_cols], r.mixers.at[here, own_cols],
            r.h_s.at[i, 2], r.h_r.at[i, 2 + j], (e, z_cross * 2 + c),
        )

    def head_relay(i, j):
        source = ((3 - d, (9 - 3 * (d + 1)) % 4)[j]) * 2 + c
        here = pl.ds(pl.multiple_of(i * wide, wide), wide)
        cols = pl.ds(pl.multiple_of(source * head_cols, head_cols), head_cols)
        return remote(
            r.mixers.at[here, cols], r.mixers.at[here, cols],
            r.h_s.at[i, 3 + j], r.h_r.at[i, 4 + j], (e, z_pair * 2 + c),
        )

    def relay_heads(first, last):
        @pl.when(outer == 0)
        def _():
            for i in range(first, last):
                for j in range(2):
                    head_cross(i, j).wait_recv()
                    head_relay(i, j).start()

    def head_forward(j):
        source = ((d + depths - j) % depths) * 2 + c
        cols = pl.ds(pl.multiple_of(source * head_cols, head_cols), head_cols)
        return remote(
            r.mixers.at[:, cols], r.mixers.at[:, cols],
            r.hf_s.at[j - 1], r.hf_r.at[j - 1], partner,
        )

    near_first = 1 + ey * (1 - ex)
    near_count = (ex + ey + 1) // 2 + ex * ey
    far_count = ey

    def tile_state(i):
        here = pl.ds(pl.multiple_of(i * wide, wide), wide)
        queries = [r.q_all[head, here, :] for head in range(heads)]
        carry = tuple(
            (r.top[head, here, :][:, :1], r.acc[head, here, :]) for head in range(heads)
        )
        return here, queries, carry

    def forward_far():
        for j in range(1, depths):
            for copy in pack_spreads(j):
                copy.wait_recv()
        for forward in pack_forwards(3):
            forward.start()

    def near_tile(i, _):
        here, queries, carry = tile_state(i)
        carry = lax.fori_loop(
            0, near_count,
            lambda s, cc: attend(
                queries, cc, pl.multiple_of((near_first + s) * rows, rows), rows, None
            ),
            carry,
        )
        for head in range(heads):
            r.top[head, here, :] = jnp.broadcast_to(carry[head][0], (wide, LANES))
            r.acc[head, here, :] = carry[head][1]

        pl.when((i == 0) & (ep_of(3) < e))(forward_far)
        return 0

    spread_slots()
    lax.fori_loop(0, 2, near_tile, 0)

    @pl.when(ep_of(3) < e)
    def _():
        for forward in pack_forwards(3):
            forward.wait_recv()
        expand(3)

    def far_tile(i, _):
        here, queries, carry = tile_state(i)
        carry = lax.fori_loop(
            0, far_count,
            lambda s, cc: attend(queries, cc, 3 * rows, rows, None),
            carry,
        )
        outs = [acc[:, NOPE : NOPE + VDIM] / acc[:, :1] for _, acc in carry]
        r.mixers[here, own_cols] = jnp.concatenate(outs, -1).astype(bf16)
        for j in (2, 1, 0):
            head_copy(i, j).start()
        return 0

    lax.fori_loop(0, 2, far_tile, 0)

    for k in (1, 2, 3):
        if k == 3:
            for j in range(1, depths):
                slot_spread(j).wait_recv()
        else:
            slot_sends(k).wait_recv()
        slot_forward(k).start()
    for name in ("eg", "eu", "ed"):
        loads[name].wait()

    quarter = width // 4
    chunks = [(n * quarter, quarter) for n in range(3)]
    chunks += [(3 * quarter, quarter // 2), (7 * quarter // 2, quarter // 2)]

    def partial_copy(n, k):
        cols = pl.ds(*chunks[n])
        at = (k if n == 0 else slice(None), slice(None), cols)
        return remote(
            r.theirs.at[at], r.pair.at[at],
            r.ex_s.at[n, k if n == 0 else 0], r.ex_r.at[n, k if n == 0 else 0], partner,
        )

    def return_copy(n, k):
        cols = pl.ds(*chunks[n])
        return remote(
            r.sums.at[k, pl.ds(0, slots), cols], r.back.at[k, pl.ds(0, slots), cols],
            r.rt_s.at[n, k - 1], r.rt_r.at[n, k - 1], (ep_of(k), t),
        )

    hidden_units = r.eg.shape[1]
    step = min(256, hidden_units)

    def expert_hidden(k):
        inputs = r.xs[k]
        for n in range(0, hidden_units, step):
            gate = silu(jnp.dot(inputs, r.eg[:, n : n + step], preferred_element_type=f32))
            up = jnp.dot(inputs, r.eu[:, n : n + step], preferred_element_type=f32)
            r.hid[k, :, n : n + step] = (gate * up).astype(bf16)

    def expert_down(n, k):
        for start, size in chunks[n : n + 1]:
            cols = slice(start, start + size)
            product = jnp.dot(
                r.hid[k], r.ed[:, cols], preferred_element_type=f32
            ).astype(bf16)
            r.ours[k, :, cols] = product[:slots]
            r.theirs[k, :, cols] = product[slots:]

    def add_pair(n, k):
        cols = slice(chunks[n][0], sum(chunks[n]))
        r.sums[k, :slots, cols] = (
            r.ours[k, :, cols].astype(f32) + r.pair[k, :, cols].astype(f32)
        ).astype(bf16)

    def first_pass(i, _):
        k = (i + 1) % 4

        @pl.when(k > 0)
        def _():
            slot_forward(k).wait_recv()

        expert_hidden(k)
        expert_down(0, k)
        partial_copy(0, k).start()

        @pl.when(i > 0)
        def _():
            partial_copy(0, i).wait_recv()
            add_pair(0, i)
            return_copy(0, i).start()

        pl.when(i == 2)(lambda: relay_heads(0, 1))
        return 0

    r.back[:, slots:, :] = jnp.zeros((4, r.back.shape[1] - slots, width), bf16)
    r.sums[0, slots:, :] = jnp.zeros((r.back.shape[1] - slots, width), bf16)
    lax.fori_loop(0, 4, first_pass, 0)

    def later_pass(n):
        def one(k, _):
            expert_down(n, k)
            return 0

        lax.fori_loop(0, 4, one, 0)
        partial_copy(n, 0).start()

    def later_sums(n):
        partial_copy(n, 0).wait_recv()

        def one(k, _):
            add_pair(n, k)
            return_copy(n, k).start()
            return 0

        lax.fori_loop(1, 4, one, 0)
        add_pair(n, 0)

    later_pass(1)
    partial_copy(0, 0).wait_recv()
    add_pair(0, 0)
    later_pass(2)
    later_sums(1)
    relay_heads(1, 2)
    later_pass(3)
    later_sums(2)
    later_pass(4)
    later_sums(3)
    later_sums(4)
    for name in ("sg", "su", "sd"):
        loads[name].wait()
    for q in range(2):
        inputs = r.nrm[q]
        hidden = silu(jnp.dot(inputs, r.sg[...], preferred_element_type=f32))
        hidden = (hidden * jnp.dot(inputs, r.su[...], preferred_element_type=f32)).astype(bf16)
        r.shared[q] = jnp.dot(hidden, r.sd[...], preferred_element_type=f32).astype(bf16)
    shared_copy = remote(r.shared.at[1], r.shared.at[2], r.sh_s, r.sh_r, partner)
    shared_copy.start()


    tags = gather_rows(0)
    routes, weight = tags[:, :top], tags[:, top : 2 * top]
    factors = [
        jnp.sum(
            jnp.where(routes == ep_of(k).astype(f32), weight, 0.0), -1, keepdims=True
        )
        for k in range(4)
    ]

    def z_copy(n, j):
        there = depth_of(j)
        cols = pl.ds(*chunks[n])
        return remote(
            r.zs.at[pl.ds(pl.multiple_of(there * MOE_DEV, MOE_DEV), MOE_DEV), cols],
            r.zr.at[j - 1, :, cols],
            r.z_s.at[n, j - 1], r.z_r.at[n, j - 1], (e, there * 2 + c),
        )

    def combine(n):
        for k in (3, 2, 1):
            return_copy(n, k).wait_recv()
        if n == 0:
            shared_copy.wait_recv()
        for start, size in chunks[n : n + 1]:
            cols = slice(start, start + size)
            total = r.shared[0, :, cols].astype(f32) + r.shared[2, :, cols].astype(f32)
            for k in range(4):
                source = r.back if k > 0 else r.sums
                total = total + factors[k] * jnp.dot(
                    r.onehot[k], source[k, :, cols], preferred_element_type=f32
                )
            r.zs[:, cols] = total.astype(bf16)
        for j in range(1, depths):
            z_copy(n, j).start()

    def mix(i, _):
        here = pl.ds(pl.multiple_of(i * tile, tile), tile)
        r.mixed[here, :] = jnp.dot(
            r.mixers[here, :], r.wo[...], preferred_element_type=f32
        ).astype(bf16)
        return 0

    combine(0)
    combine(1)
    combine(2)
    for i in range(2):
        head_copy(i, 1).wait_recv()

    @pl.when(outer == 1)
    def _():
        for i in range(2):
            for j in range(2):
                head_relay(i, j).wait_recv()

    for j in range(1, depths):
        head_forward(j).start()
    combine(3)
    combine(4)
    loads["wo"].wait()
    for i in range(2):
        head_copy(i, 0).wait_recv()
    for j in range(1, depths):
        head_forward(j).wait_recv()
    lax.fori_loop(0, 4, mix, 0)
    for n in range(len(chunks)):
        for j in range(1, depths):
            z_copy(n, j).wait_recv()
    final = r.zs[pl.ds(pl.multiple_of(d * MOE_DEV, MOE_DEV), MOE_DEV), :].astype(f32)
    for j in range(1, depths):
        final = final + r.zr[j - 1].astype(f32)
    r.moe_out[...] = final.astype(bf16)

    for k in (1, 2, 3):

        @pl.when(ep_of(k) > e)
        def _(k=k):
            for copy in pack_copies(k):
                copy.wait_send()

        @pl.when(ep_of(k) < e)
        def _(k=k):
            for copy in pack_forwards(k):
                copy.wait_send()
            if k == 3:
                for j in range(1, depths):
                    for copy in pack_spreads(j):
                        copy.wait_send()

        slot_sends(k).wait_send()
        slot_forward(k).wait_send()
        for n in range(len(chunks)):
            return_copy(n, k).wait_send()
    shared_copy.wait_send()
    rows_copy.wait_send()
    for k in range(4):
        partial_copy(0, k).wait_send()
    for n in range(1, len(chunks)):
        partial_copy(n, 0).wait_send()
    for i in range(2):
        for j in range(3):
            head_copy(i, j).wait_send()

    @pl.when(outer == 0)
    def _():
        for i in range(2):
            for j in range(2):
                head_relay(i, j).wait_send()

    for j in range(1, depths):
        slot_spread(j).wait_send()
        head_forward(j).wait_send()
        for n in range(len(chunks)):
            z_copy(n, j).wait_send()


def rotary_constant(total, per_device):
    halfway = ROPE_DIM // 2
    inverse = (
        np.float32(rotary_base)
        ** (-(np.arange(halfway, dtype=np.float32) * np.float32(2.0) / np.float32(ROPE_DIM)))
    ).astype(np.float32)
    angles = (np.arange(total, dtype=np.float32)[:, None] * inverse[None, :]).astype(np.float32)
    angles = angles.astype(np.float64)
    both = np.concatenate([np.cos(angles), np.sin(angles)], 1).astype(np.float32)
    groups = both.reshape(-1, LANES // ROPE_DIM, per_device * ROPE_DIM // LANES, ROPE_DIM)
    return groups.transpose(0, 2, 1, 3).reshape(-1, LANES)


def fused_body(
    q_latent,
    kv_latent,
    rope_key,
    q_gain,
    kv_gain,
    w_query,
    w_keyval,
    w_output,
    moe_input,
    moe_gain,
    routes,
    route_weight,
    expert_gate,
    expert_up,
    expert_down,
    shared_gate,
    shared_up,
    shared_down,
):
    rows, qlat = q_latent.shape
    latent = kv_latent.shape[1]
    ep_count = lax.axis_size("ep")
    tp_count = lax.axis_size("tp")
    heads = w_query.shape[1] // (NOPE + ROPE_DIM)
    tokens, width = moe_input.shape
    side = tokens // 2
    depths = tp_count // 2
    hidden = expert_gate.shape[2]
    shared_hidden = shared_gate.shape[1]
    top = routes.shape[1]
    capacity = 3 * MOE_DEV * top // (2 * ep_count)
    slots = depths * capacity
    columns = w_output.shape[1]
    bf16, f32 = jnp.bfloat16, jnp.float32
    table = jnp.asarray(rotary_constant(rows * ep_count, rows))
    hbm = pl.BlockSpec(memory_space=pltpu.HBM)
    vmem = pl.BlockSpec(memory_space=pltpu.VMEM)
    inputs = [
        ("q_hbm", q_latent, hbm),
        ("kv_hbm", kv_latent, hbm),
        ("table_hbm", table, hbm),
        ("moe_hbm", moe_input, hbm),
        ("eg_hbm", expert_gate, hbm),
        ("eu_hbm", expert_up, hbm),
        ("ed_hbm", expert_down, hbm),
        ("sg_hbm", shared_gate, hbm),
        ("su_hbm", shared_up, hbm),
        ("sd_hbm", shared_down, hbm),
        ("wo_hbm", w_output, hbm),
        ("rope_t", rope_key.T, vmem),
        ("q_gain", q_gain.reshape(1, -1), vmem),
        ("kv_gain", kv_gain.reshape(1, -1), vmem),
        ("wq_t", w_query.T, vmem),
        ("wkv", w_keyval, vmem),
        ("moe_gain", moe_gain.reshape(1, -1), vmem),
        ("routes_t", routes.T, vmem),
        ("weight_t", route_weight.T, vmem),
    ]
    outputs = [("mixed", (rows, columns)), ("moe_out", (MOE_DEV, width))]
    dma = pltpu.SemaphoreType.DMA
    scratch = [
        ("kv_raw", pltpu.VMEM((rows, latent), bf16)),
        ("q_raw", pltpu.VMEM((rows, qlat), bf16)),
        ("table", pltpu.VMEM((rows // 4, LANES), f32)),
        ("tags", pltpu.VMEM((LANES, tokens), f32)),
        ("tagged", pltpu.VMEM((tokens, LANES), f32)),
        ("wq", pltpu.VMEM((qlat, heads * LANES), bf16)),
        ("cosine", pltpu.VMEM((rows, LANES), f32)),
        ("sine", pltpu.VMEM((rows, LANES), f32)),
        ("kvs", pltpu.VMEM((4, rows, latent), bf16)),
        ("ropes", pltpu.VMEM((4, 2, rows // 8, LANES), bf16)),
        ("nrm", pltpu.VMEM((2, side, width), bf16)),
        ("onehot", pltpu.VMEM((4, side, LANES), bf16)),
        ("snd", pltpu.VMEM((3, slots, width), bf16)),
        ("xs", pltpu.VMEM((4, 2 * slots, width), bf16)),
        ("shared", pltpu.VMEM((3, side, width), bf16)),
        ("q_all", pltpu.VMEM((heads, rows, LANES), bf16)),
        ("k_all", pltpu.VMEM((heads, 4 * rows, LANES), bf16)),
        ("v_all", pltpu.VMEM((heads, 4 * rows, LANES), bf16)),
        ("top", pltpu.VMEM((heads, rows, LANES), f32)),
        ("acc", pltpu.VMEM((heads, rows, LANES), f32)),
        ("mixers", pltpu.VMEM((rows, tp_count * heads * VDIM), bf16)),
        ("ours", pltpu.VMEM((4, slots, width), bf16)),
        ("theirs", pltpu.VMEM((4, slots, width), bf16)),
        ("pair", pltpu.VMEM((4, slots, width), bf16)),
        ("sums", pltpu.VMEM((4, LANES, width), bf16)),
        ("hid", pltpu.VMEM((4, 2 * slots, hidden), bf16)),
        ("back", pltpu.VMEM((4, LANES, width), bf16)),
        ("zs", pltpu.VMEM((side, width), bf16)),
        ("zr", pltpu.VMEM((depths - 1, MOE_DEV, width), bf16)),
        ("eg", pltpu.VMEM((width, hidden), bf16)),
        ("eu", pltpu.VMEM((width, hidden), bf16)),
        ("ed", pltpu.VMEM((hidden, width), bf16)),
        ("sg", pltpu.VMEM((width, shared_hidden), bf16)),
        ("su", pltpu.VMEM((width, shared_hidden), bf16)),
        ("sd", pltpu.VMEM((shared_hidden, width), bf16)),
        ("wo", pltpu.VMEM(w_output.shape, bf16)),
        ("ld", dma((10 + depths,))),
        ("pk_s", dma((3, 2))),
        ("pk_r", dma((3, 2))),
        ("pf_s", dma((3, 2))),
        ("pf_r", dma((3, 2))),
        ("sl_s", dma((3,))),
        ("sl_r", dma((3,))),
        ("ps_s", dma((depths - 1, 2))),
        ("ps_r", dma((depths - 1, 2))),
        ("ss_s", dma((depths - 1,))),
        ("ss_r", dma((depths - 1,))),
        ("sf_s", dma((3,))),
        ("sf_r", dma((3,))),
        ("rc_s", dma),
        ("rc_r", dma),
        ("sh_s", dma),
        ("sh_r", dma),
        ("ex_s", dma((5, 4))),
        ("ex_r", dma((5, 4))),
        ("rt_s", dma((5, 3))),
        ("rt_r", dma((5, 3))),
        ("h_s", dma((2, 5))),
        ("h_r", dma((2, 6))),
        ("hf_s", dma((depths - 1,))),
        ("hf_r", dma((depths - 1,))),
        ("z_s", dma((5, depths - 1))),
        ("z_r", dma((5, depths - 1))),
    ]
    names = [x[0] for x in inputs] + [x[0] for x in outputs] + [x[0] for x in scratch]
    mixed, moe_out = pl.pallas_call(
        lambda *refs: fused_kernel(names, *refs),
        out_shape=[jax.ShapeDtypeStruct(shape, bf16) for _, shape in outputs],
        in_specs=[spec for _, _, spec in inputs],
        out_specs=[vmem] * len(outputs),
        scratch_shapes=[spec for _, spec in scratch],
        compiler_params=pltpu.CompilerParams(
            collective_id=0,
            has_side_effects=True,
            vmem_limit_bytes=60 * 1024 * 1024,
        ),
        name="fused",
    )(*[value for _, value, _ in inputs])
    return (mixed, moe_out)


def solution(mesh):
    in_specs = (
        P("ep", None),
        P("ep", None),
        P("ep", None),
        P(),
        P(),
        P(None, "tp"),
        P(None, "tp"),
        P(None, "tp"),
        P("ep", None),
        P(),
        P("ep", None),
        P("ep", None),
        P("ep", None, "tp"),
        P("ep", None, "tp"),
        P("ep", "tp", None),
        P(None, "tp"),
        P(None, "tp"),
        P("tp", None),
    )
    out_specs = (P("ep", "tp"), P(("ep", "tp"), None))
    chosen = fused_body if (mesh.shape["ep"], mesh.shape["tp"]) == (4, 8) else body
    return jax.shard_map(
        chosen, mesh=mesh, in_specs=in_specs, out_specs=out_specs, check_vma=False
    )
```
